32 devices in a mesh: grp: 2 (over y), fs: 4 (over z), tp: 4 (over x, core).
Axes of the slice: x: 2, y: 2, z: 4, core: 2. Of those that a mesh axis runs over, the one named last changes fastest.
Arguments:
- tokens: bfloat16 [32, 128, 2048], P(('grp', 'fs'), None, 'tp'), parts along dimension 0, may hold values from -100 to 100
- mix_gain: float32 [2048], replicated, may hold values from 0.1 to 1.9
- gate_outer: bfloat16 [2048, 1024], P('fs', 'tp'), may hold values from -0.125 to 0.125
- gate_inner: bfloat16 [2048, 1024], P('fs', 'tp'), may hold values from -0.125 to 0.125
- value_weight: bfloat16 [2048, 1024], P('fs', 'tp'), may hold values from -0.125 to 0.125
- conv_taps: float32 [3, 1024], replicated, may hold values from -3 to 3
- mix_out: bfloat16 [1024, 2048], P('tp', 'fs'), may hold values from -0.25 to 0.25
- ffn_gain: float32 [2048], replicated, may hold values from 0.1 to 1.9
- ffn_gate: bfloat16 [2048, 5632], P('fs', 'tp'), may hold values from -0.125 to 0.125
- ffn_up: bfloat16 [2048, 5632], P('fs', 'tp'), may hold values from -0.125 to 0.125
- ffn_down: bfloat16 [5632, 2048], P('tp', 'fs'), may hold values from -0.109375 to 0.109375
- out_gain: float32 [2048], replicated, may hold values from 0.1 to 1.9
Outputs:
- layer_out: bfloat16 [32, 128, 2048], P(('grp', 'fs'), None, 'tp'), parts along dimension 0
The draws below stay inside these ranges and needn't reach their ends.
There are 2 independent parts, one for each index of `grp`. The reference program is written for one: setup_inputs(seed, part) draws one part's arguments, and reference() takes and returns one part's arrays. A program takes and returns all parts, laid end to end along the dimension named above; an argument that names none is the same for every part. Nothing has to cross between parts.
All inputs are finite; a program needn't handle non-finite values.
Results may differ from the reference program's by a relative error of at most 0.015.
Values may be sent and summed in bfloat16 or wider, within the bound.
A program may use at most 64 MiB of HBM per device.

```python
import math
import jax
import jax.numpy as jnp
from jax import lax

D = 2048
CA = 1024
FF = 5632
TAPS = 3
LEN = 128
SEQS = 16
N_TP = 4


def draw_tokens(key, part):
    first_key, second_key = jax.random.split(jax.random.fold_in(key, 11), 2)
    ramp = jnp.exp(jnp.linspace(math.log(0.4), math.log(4.0), D)).astype(jnp.float32)
    rough = jax.random.uniform(second_key, (D,), jnp.float32, 0.6, 1.4)
    values = jax.random.normal(first_key, (SEQS, LEN, D), jnp.float32) * ramp * rough
    return jnp.clip(values, -100.0, 100.0).astype(jnp.bfloat16)


def with_spikes(drawn, own_key, source, target, parts, factor):
    owner, partner = [(jnp.arange(drawn.shape[dim]) // (drawn.shape[dim] // parts)).reshape([-1 if axis == dim else 1 for axis in range(drawn.ndim)]) for dim in (source, target)]
    chosen = jax.random.permutation(own_key, parts)[partner]
    strong = (owner == chosen) | (owner == (partner + parts // 2) % parts)
    return jnp.where(strong, factor * drawn, drawn)


def block_levels(stream_key, dims, cuts, low, largest):
    factor_of, own = 1.0, jax.random.fold_in(stream_key, 6)
    for axis_at, shards_of in cuts:
        draws = jnp.exp(jax.random.uniform(jax.random.fold_in(own, axis_at), (shards_of,), jnp.float32, low / len(cuts), largest / len(cuts)))
        factor_of = factor_of * jnp.repeat(draws, dims[axis_at] // shards_of).reshape([-1 if axis == axis_at else 1 for axis in range(len(dims))])
    return factor_of


def centred(own_key, dims, spread, limit, cuts=(), held_as=jnp.bfloat16):
    values = spread * jax.random.normal(own_key, dims, jnp.float32)
    if cuts:
        values = values * block_levels(own_key, dims, cuts, -0.22, 0.18)
    return jnp.clip(values, -limit, limit).astype(held_as)


def gaussian_with(key, extent, scale, limit, pieces, heavy, held_as=jnp.bfloat16):
    result = scale * jax.random.normal(key, extent, jnp.float32)
    if pieces:
        result = result * block_levels(key, extent, pieces, -0.22, 0.18)
    return jnp.clip(with_spikes(result, jax.random.fold_in(key, 3), *heavy), -limit, limit).astype(held_as)


def setup_inputs(seed: int = 0, part: int = 0) -> dict:
    streams_of = jax.random.split(jax.random.key(seed), 13)
    part_splits = jax.random.split(jax.random.fold_in(streams_of[12], part), 13)
    return {
        "tokens": draw_tokens(jax.random.fold_in(jax.random.fold_in(streams_of[12], part), 71), part),
        "mix_gain": jnp.clip(1.0 + 0.18 * jax.random.normal(streams_of[1], (D,), jnp.float32), 0.1, 1.9),
        "gate_outer": centred(streams_of[2], (D, CA), D ** -0.5, 0.125, ((0, 4), (1, 4))),
        "gate_inner": centred(streams_of[3], (D, CA), D ** -0.5, 0.125, ((0, 4), (1, 4))),
        "value_weight": centred(streams_of[4], (D, CA), D ** -0.5, 0.125, ((0, 4), (1, 4))),
        "conv_taps": centred(streams_of[5], (TAPS, CA), 0.6, 3.0, (), jnp.float32),
        "mix_out": gaussian_with(streams_of[6], (CA, D), CA ** -0.5, 0.25, ((0, 4), (1, 4)), (0, 1, 4, 2.0)),
        "ffn_gain": jnp.clip(1.0 + 0.18 * jax.random.normal(streams_of[7], (D,), jnp.float32), 0.1, 1.9),
        "ffn_gate": centred(streams_of[8], (D, FF), D ** -0.5, 0.125, ((0, 4), (1, 4))),
        "ffn_up": centred(streams_of[9], (D, FF), D ** -0.5, 0.125, ((0, 4), (1, 4))),
        "ffn_down": gaussian_with(streams_of[10], (FF, D), FF ** -0.5, 0.109375, ((0, 4), (1, 4)), (0, 1, 4, 2.0)),
        "out_gain": jnp.clip(1.0 + 0.18 * jax.random.normal(streams_of[11], (D,), jnp.float32), 0.1, 1.9),
    }


def rms_norm(values, gain):
    floats = values.astype(jnp.float32)
    scaled = floats * lax.rsqrt(lax.optimization_barrier(jnp.mean(floats * floats, axis=-1, keepdims=True)) + 1e-06)
    return scaled * gain.astype(jnp.float32)

def blocked_sum(left, weight, blocks):
    width = left.shape[1] // blocks
    summed = jnp.zeros((left.shape[0], weight.shape[1]), jnp.float32)
    for number in range(blocks):
        partial_value = jnp.dot(left[:, number * width:(number + 1) * width], weight[number * width:(number + 1) * width], preferred_element_type=jnp.float32).astype(jnp.bfloat16)
        summed = summed + lax.optimization_barrier(partial_value).astype(jnp.float32)
    return summed

def reference(tokens, mix_gain, gate_outer, gate_inner, value_weight, conv_taps, mix_out, ffn_gain, ffn_gate, ffn_up, ffn_down, out_gain):
    rows = SEQS * LEN
    flat = tokens.reshape(rows, D)
    normed = rms_norm(flat, mix_gain).astype(jnp.bfloat16)
    outer = jnp.dot(normed, gate_outer, preferred_element_type=jnp.float32).astype(jnp.bfloat16)
    inner = jnp.dot(normed, gate_inner, preferred_element_type=jnp.float32).astype(jnp.bfloat16)
    values = jnp.dot(normed, value_weight, preferred_element_type=jnp.float32).astype(jnp.bfloat16)
    product = (inner.astype(jnp.float32) * values.astype(jnp.float32)).reshape(SEQS, LEN, CA)
    padded = jnp.pad(product, ((0, 0), (TAPS - 1, 0), (0, 0)))
    conv = jnp.zeros((SEQS, LEN, CA), jnp.float32)
    for offset in range(TAPS):
        conv = conv + conv_taps[offset].astype(jnp.float32) * padded[:, offset:offset + LEN]
    gated = (outer.astype(jnp.float32) * conv.reshape(rows, CA)).astype(jnp.bfloat16)
    first = (flat.astype(jnp.float32) + blocked_sum(gated, mix_out, N_TP)).astype(jnp.bfloat16)
    normed_ffn = rms_norm(first, ffn_gain).astype(jnp.bfloat16)
    gate = jnp.dot(normed_ffn, ffn_gate, preferred_element_type=jnp.float32)
    upward = jnp.dot(normed_ffn, ffn_up, preferred_element_type=jnp.float32)
    hidden = (jax.nn.silu(gate) * upward).astype(jnp.bfloat16)
    second = first.astype(jnp.float32) + blocked_sum(hidden, ffn_down, N_TP)
    return rms_norm(second, out_gain).astype(jnp.bfloat16).reshape(SEQS, LEN, D)
```

```python
import functools

import jax
import jax.numpy as jnp
from jax import lax
from jax.experimental import pallas as pl
from jax.experimental.pallas import tpu as pltpu
from jax.sharding import PartitionSpec as P

MESH = pl.DeviceIdType.MESH
F32 = jnp.float32
BF16 = jnp.bfloat16
MIXER = 4
GATE, UP, DOWN = 4, 5, 6
SHARED = 2
LAG = 2


def tiles_of(units):
    if units % 128:
        return ((0, units),)
    return tuple((start, min(256, units - start)) for start in range(0, units, 256))


def column(rows):
    wide = jnp.broadcast_to(rows, (rows.shape[1], rows.shape[1]))
    return jnp.transpose(wide)[:, :1]


def kernel(
    n, parts, n_tp, length, spans,
    tok_ref, mix_gain, w0, w1, w2, taps_ref, w3, ffn_gain, w4, w5, w6, out_gain,
    out_ref,
    f0, f1, f2, f3, f4, f5, f6,
    tok_full, normed, proj, gated, part, pair_recv, far_recv, first_full, hidden, returned, second_own, sq_acc,
    sq_send, sq_recv, sq_total, sq_back,
    z_send, z_recv, y_send, y_recv, own_sem, pair_ss, pair_rs, far_ss, far_rs,
    down_pair_ss, down_pair_rs, down_far_ss, down_far_rs, sq_ss, sq_rs, back_ss, back_rs, guest_sem,
):
    own = (w0, w1, w2, w3, w4, w5, w6)
    full = (f0, f1, f2, f3, f4, f5, f6)
    f, g, t = lax.axis_index("fs"), lax.axis_index("grp"), lax.axis_index("tp")
    rows, columns = tok_ref.shape
    width = columns * n_tp
    seqs = rows // length
    counts = [len(tiles) for tiles in spans]
    bases = [sum(counts[:w]) for w in range(7)]

    def y_peer(k):
        return lax.rem(g + k, parts)

    def tp_peer(k):
        return lax.rem(t + k, n_tp)

    def span(w, half, c):
        size = own[w].shape[0] // parts
        if isinstance(c, int):
            at = pl.ds(*spans[w][c])
        else:
            width_c = spans[w][0][1]
            at = pl.ds(pl.multiple_of(c * width_c, 128), width_c)
        return pl.ds(pl.multiple_of(half * size, 8), size), at

    def region(w, blk, half, c):
        at_rows, at_cols = span(w, half, c)
        return full[w].at[blk, at_rows, at_cols]

    def piece_of(w, half, c):
        at_rows, at_cols = span(w, half, c)
        return own[w].at[at_rows, at_cols]

    barrier = pltpu.get_barrier_semaphore()
    for k in range(1, n_tp):
        pl.semaphore_signal(barrier, inc=1, device_id={"tp": tp_peer(k)}, device_id_type=MESH)
    for k in range(1, parts):
        pl.semaphore_signal(barrier, inc=1, device_id={"grp": y_peer(k)}, device_id_type=MESH)

    @pl.when(f < n - 1)
    def _():
        pl.semaphore_signal(barrier, inc=1, device_id={"fs": f + 1}, device_id_type=MESH)

    @pl.when(f > 0)
    def _():
        pl.semaphore_signal(barrier, inc=1, device_id={"fs": f - 1}, device_id_type=MESH)

    neighbours = lax.min(f, 1) + lax.min(n - 1 - f, 1)
    pl.semaphore_wait(barrier, n_tp - 1 + parts - 1 + neighbours)

    def z_slot(blk, step):
        return lax.select((blk == f) & (step < 0), n, blk)

    def half_block(w, blk):
        size = own[w].shape[0] // parts
        return full[w].at[blk, pl.ds(pl.multiple_of(g * size, 8), size), :]

    def z_sent(w, blk, step):
        half = half_block(w, blk)
        pltpu.make_async_remote_copy(
            src_ref=half, dst_ref=half, send_sem=z_send.at[w, z_slot(blk, step)], recv_sem=z_recv.at[bases[w], blk],
            device_id={"fs": f + step}, device_id_type=MESH,
        ).wait_send()

    def y_sent(w, blk, k):
        half = half_block(w, blk)
        pltpu.make_async_remote_copy(
            src_ref=half, dst_ref=half, send_sem=y_send.at[w, blk, k - 1], recv_sem=y_recv.at[bases[w], blk, k - 1],
            device_id={"grp": y_peer(k)}, device_id_type=MESH,
        ).wait_send()

    def z_copy(w, c, blk, src, step):
        return pltpu.make_async_remote_copy(
            src_ref=src, dst_ref=region(w, blk, g, c),
            send_sem=z_send.at[w, z_slot(blk, step)], recv_sem=z_recv.at[bases[w] + c, blk],
            device_id={"fs": f + step}, device_id_type=MESH,
        )

    def y_copy(w, c, blk, half, k, peer):
        return pltpu.make_async_remote_copy(
            src_ref=region(w, blk, half, c), dst_ref=region(w, blk, half, c),
            send_sem=y_send.at[w, blk, k - 1], recv_sem=y_recv.at[bases[w] + c, blk, k - 1],
            device_id={"grp": peer}, device_id_type=MESH,
        )

    first_host, last_host = 1, n - 2
    is_host = (f >= first_host) & (f <= last_host)
    inner = lax.select(2 * f + 1 < n, 1, -1)

    def start_own(w, c):
        src = piece_of(w, g, c)

        @pl.when(f + 1 <= last_host)
        def _():
            z_copy(w, c, f, src, 1).start()

        @pl.when(f - 1 >= first_host)
        def _():
            z_copy(w, c, f, src, -1).start()

    def other_half(w, c, k):
        half = lax.rem(g + parts - k, parts)
        inward = lax.select(f == 0, 1, n - 2)
        return pltpu.make_async_remote_copy(
            src_ref=piece_of(w, half, c), dst_ref=region(w, f, half, c),
            send_sem=y_send.at[w, f, k - 1], recv_sem=y_recv.at[bases[w] + c, f, k - 1],
            device_id={"fs": inward}, device_id_type=MESH,
        )

    def direct(w):
        return w >= SHARED

    def relay(w, c, s, toward, next_to_edge):
        blk = f + toward * (1 + s)
        step = -toward

        @pl.when((blk >= 0) & (blk < n))
        def _():
            z_copy(w, c, blk, region(w, blk, g, c), step).wait_recv()

            def share():
                for k in range(1, parts):
                    y_copy(w, c, blk, g, k, y_peer(k)).start()

            def onward():
                z_copy(w, c, blk, region(w, blk, g, c), step).start()

            pl.when((f + step <= last_host) & (f + step >= first_host))(onward)
            if next_to_edge and direct(w):
                pl.when((blk > 0) & (blk < n - 1))(share)
            else:
                share()

    def from_inner(w, c):
        relay(w, c, 0, inner, True)

    def from_outer(w, c):
        relay(w, c, 0, -inner, True)

    def from_far(w, c):
        @pl.loop(1, n - 2)
        def _(s):
            relay(w, c, s, inner, False)
            relay(w, c, s, -inner, False)

    def finish(w, c, blk):
        for k in range(1, parts):
            source = lax.rem(g + parts - k, parts)
            y_copy(w, c, blk, source, k, source).wait_recv()

    def finish_all(w, c):
        @pl.loop(0, n)
        def _(blk):
            pl.when(blk != f)(lambda: finish(w, c, blk))

    def own_copy(w):
        return pltpu.make_async_copy(own[w], full[w].at[f], own_sem.at[w])

    def own_columns(owner):
        return pl.ds(pl.multiple_of(owner * columns, 128), columns)

    chips = n_tp // 2
    core = lax.rem(t, 2)
    pair = t + 1 - 2 * core

    def ahead(k, start=None):
        return lax.rem((t if start is None else start) + 2 * k, n_tp)

    def behind(k, start=None):
        return lax.rem((t if start is None else start) + n_tp - 2 * k, n_tp)

    def set_rows(r):
        return pl.ds(r * rows, rows)

    def pair_copy(stage, r, k, src, dst):
        return pltpu.make_async_remote_copy(
            src_ref=src, dst_ref=dst, send_sem=pair_ss.at[stage, r, k], recv_sem=pair_rs.at[stage, r, k],
            device_id={"tp": pair}, device_id_type=MESH,
        )

    def far_copy(stage, r, k, src, dst, peer):
        return pltpu.make_async_remote_copy(
            src_ref=src, dst_ref=dst, send_sem=far_ss.at[stage, r, k], recv_sem=far_rs.at[stage, r, k],
            device_id={"tp": peer}, device_id_type=MESH,
        )

    def block_of(buf, r, owner):
        return buf.at[set_rows(r), own_columns(owner)]

    def gather_send(buf, stage, r):
        mine = block_of(buf, r, t)
        for k in range(1, chips):
            far_copy(stage, r, k, mine, mine, ahead(k)).start()
        pair_copy(stage, r, 0, mine, mine).start()

    def gather_relay(buf, stage, r):
        for k in range(1, chips):
            theirs = block_of(buf, r, behind(k))
            far_copy(stage, r, k, theirs, theirs, behind(k)).wait_recv()
            pair_copy(stage, r, k, theirs, theirs).start()

    def gather_finish(buf, stage, r):
        for k in range(chips):
            theirs = block_of(buf, r, behind(k, pair))
            pair_copy(stage, r, k, theirs, theirs).wait_recv()

    def gather_sent(buf, stage, r):
        mine = block_of(buf, r, t)
        for k in range(1, chips):
            far_copy(stage, r, k, mine, mine, ahead(k)).wait_send()
        for k in range(chips):
            pair_copy(stage, r, k, mine, mine).wait_send()

    def to_pair(r, k):
        return pair_copy(1, r, k, block_of(part, r, ahead(k, pair)), pair_recv.at[r, k])

    def to_far(r, k):
        return far_copy(1, r, k, block_of(part, r, ahead(k)), far_recv.at[r, k], ahead(k))

    def sum_send(r):
        for k in range(chips - 1, -1, -1):
            to_pair(r, k).start()

    def sum_relay(r):
        for k in range(1, chips):
            to_pair(r, k).wait_recv()

            @pl.loop(0, rows // 64)
            def _(i):
                inside = pl.ds(pl.multiple_of(i * 64, 64), 64)
                at = pl.ds(pl.multiple_of(r * rows + i * 64, 64), 64)
                both = part[at, own_columns(ahead(k))].astype(F32) + pair_recv[r, k, inside, :].astype(F32)
                part[at, own_columns(ahead(k))] = both.astype(BF16)

            to_far(r, k).start()

    def summed(r, start, size):
        inside = pl.ds(pl.multiple_of(start, size), size)
        at = pl.ds(pl.multiple_of(r * rows + start, size), size)
        total = part[at, own_columns(t)].astype(F32) + pair_recv[r, 0, inside, :].astype(F32)
        for k in range(1, chips):
            total = total + far_recv[r, k, inside, :].astype(F32)
        return at, total

    def first_rows(r):
        to_pair(r, 0).wait_recv()
        for k in range(1, chips):
            to_far(r, k).wait_recv()

        @pl.loop(0, rows // 64)
        def _(i):
            at, total = summed(r, i * 64, 64)
            first_full[at, own_columns(t)] = (tok_full[at, own_columns(t)].astype(F32) + total).astype(BF16)

    def norm_rows(source, gain, r):
        size = 32

        @pl.loop(0, rows // size)
        def _(i):
            at = pl.ds(pl.multiple_of(r * rows + i * size, size), size)
            values = source[at, :].astype(F32)
            scale = lax.rsqrt(jnp.sum(values * values, axis=1, keepdims=True) / width + 1e-06)
            normed[at, :] = (values * scale * gain[...]).astype(BF16)

    channels = w0.shape[1]
    block = w3.shape[1]
    units = w4.shape[1]
    tap_count = taps_ref.shape[0]

    def mixer(r):
        for w in range(3):
            weight = full[w][...].reshape(width, channels)
            proj[w] = jnp.dot(normed[set_rows(r), :], weight, preferred_element_type=F32).astype(BF16)
        taps = taps_ref[:, pl.ds(pl.multiple_of(t * channels, 128), channels)]

        @pl.loop(0, seqs)
        def _(i):
            at = pl.ds(pl.multiple_of(i * length, length), length)
            product = proj[1, at, :].astype(F32) * proj[2, at, :].astype(F32)
            position = lax.broadcasted_iota(jnp.int32, product.shape, 0)
            conv = jnp.zeros_like(product)
            for offset in range(tap_count):
                shift = tap_count - 1 - offset
                moved = product if shift == 0 else jnp.where(position >= shift, pltpu.roll(product, shift, 0), 0.0)
                conv = conv + taps[offset : offset + 1, :] * moved
            gated[at, :] = (proj[0, at, :].astype(F32) * conv).astype(BF16)

        @pl.loop(0, n)
        def _(b):
            at = pl.ds(pl.multiple_of(b * block, 128), block)
            part[set_rows(r), at] = jnp.dot(gated[...], full[3][b], preferred_element_type=F32).astype(BF16)

    def hidden_tile(r, start, size):
        at = pl.ds(start, size)
        left = normed[set_rows(r), :]
        gate = jnp.dot(left, full[GATE][:, :, at].reshape(width, size), preferred_element_type=F32)
        upward = jnp.dot(left, full[UP][:, :, at].reshape(width, size), preferred_element_type=F32)
        hidden[set_rows(r), at] = (gate / (1.0 + jnp.exp(-gate)) * upward).astype(BF16)

    def hidden_tiles(c, r):
        first, total = spans[GATE][c]
        for offset in range(0, total, 256):
            hidden_tile(r, first + offset, min(256, total - offset))

    wide = w6.shape[1]
    piece = spans[DOWN][0][1]
    pieces = counts[DOWN]

    def down_to_pair(r, k, slot, start):
        inside = pl.ds(pl.multiple_of(slot * piece, 128), piece)
        return pltpu.make_async_remote_copy(
            src_ref=part.at[set_rows(r), pl.ds(start, piece)], dst_ref=pair_recv.at[r, k, :, inside],
            send_sem=down_pair_ss.at[r, k], recv_sem=down_pair_rs.at[r, k, slot],
            device_id={"tp": pair}, device_id_type=MESH,
        )

    def down_to_far(r, k, slot, start):
        inside = pl.ds(pl.multiple_of(slot * piece, 128), piece)
        return pltpu.make_async_remote_copy(
            src_ref=part.at[set_rows(r), pl.ds(start, piece)], dst_ref=far_recv.at[r, k, :, inside],
            send_sem=down_far_ss.at[r, k], recv_sem=down_far_rs.at[r, k, slot],
            device_id={"tp": lax.rem(t + 2 * k, n_tp)}, device_id_type=MESH,
        )

    def down_sent(r, k):
        whole = pair_recv.at[r, k]
        pltpu.make_async_remote_copy(
            src_ref=whole, dst_ref=whole, send_sem=down_pair_ss.at[r, k], recv_sem=down_pair_rs.at[r, k, 0],
            device_id={"tp": pair}, device_id_type=MESH,
        ).wait_send()
        if k > 0:
            pltpu.make_async_remote_copy(
                src_ref=whole, dst_ref=whole, send_sem=down_far_ss.at[r, k], recv_sem=down_far_rs.at[r, k, 0],
                device_id={"tp": lax.rem(t + 2 * k, n_tp)}, device_id_type=MESH,
            ).wait_send()

    def place(b, c):
        start = pl.multiple_of(b * wide + c * piece, 128)
        owner = (b * wide + c * piece) // columns
        slot = lax.rem(b * wide + c * piece, columns) // piece
        k = lax.rem(owner // 2 - t // 2 + chips, chips)
        return start, owner, slot, k, lax.rem(owner, 2) == core

    def down_product(b, offset, size):
        at_cols = pl.ds(pl.multiple_of(b * wide + offset, 128), size)

        @pl.loop(0, 2)
        def _(turn):
            r = 1 - turn
            at = pl.ds(pl.multiple_of(r * rows, rows), rows)
            weight = full[DOWN][b, :, pl.ds(offset, size)]
            part[at, at_cols] = jnp.dot(hidden[at, :], weight, preferred_element_type=F32).astype(BF16)

    def to_lane(b, c):
        start, owner, slot, k, lane = place(b, c)

        @pl.when(jnp.logical_not(lane))
        def _():
            for r in (1, 0):
                down_to_pair(r, k, slot, start).start()

    def combine(b, c):
        start, owner, slot, k, lane = place(b, c)

        @pl.when(lane & (k > 0))
        def _():
            inside = pl.ds(pl.multiple_of(slot * piece, 128), piece)
            for r in (1, 0):
                down_to_pair(r, k, slot, start).wait_recv()

                @pl.loop(0, rows // 64)
                def _(i):
                    here = pl.ds(pl.multiple_of(i * 64, 64), 64)
                    at = pl.ds(pl.multiple_of(r * rows + i * 64, 64), 64)
                    both = part[at, pl.ds(start, piece)].astype(F32) + pair_recv[r, k, here, inside].astype(F32)
                    part[at, pl.ds(start, piece)] = both.astype(BF16)

                down_to_far(r, k, slot, start).start()

    def back_copy(slot, device):
        at = pl.ds(pl.multiple_of(slot * piece, 128), piece)
        return pltpu.make_async_remote_copy(
            src_ref=returned.at[:, at], dst_ref=returned.at[:, at], send_sem=back_ss.at[0], recv_sem=back_rs.at[slot],
            device_id={"fs": device}, device_id_type=MESH,
        )

    def back_sent():
        pltpu.make_async_remote_copy(
            src_ref=returned, dst_ref=returned, send_sem=back_ss.at[0], recv_sem=back_rs.at[0],
            device_id={"fs": guest}, device_id_type=MESH,
        ).wait_send()

    def settle(b, c):
        start, owner, slot, k, lane = place(b, c)

        @pl.when(owner == t)
        def _():
            inside = pl.ds(pl.multiple_of(slot * piece, 128), piece)
            for r in (1, 0):
                down_to_pair(r, 0, slot, start).wait_recv()
                for far in range(1, chips):
                    down_to_far(r, far, slot, start).wait_recv()

                @pl.loop(0, rows // 64)
                def _(i):
                    here = pl.ds(pl.multiple_of(i * 64, 64), 64)
                    at = pl.ds(pl.multiple_of(r * rows + i * 64, 64), 64)
                    total = part[at, pl.ds(start, piece)].astype(F32) + pair_recv[r, 0, here, inside].astype(F32)
                    for far in range(1, chips):
                        total = total + far_recv[r, far, here, inside].astype(F32)
                    second = first_full[at, pl.ds(start, piece)].astype(F32) + total
                    squares = second * second
                    folded = squares[:, :128]
                    for lane_block in range(1, piece // 128):
                        folded = folded + squares[:, lane_block * 128 : (lane_block + 1) * 128]
                    sq_acc[at, :] += folded
                    if r == 0:
                        second_own[here, inside] = second
                    else:
                        returned[here, inside] = second.astype(BF16)

                if r == 1:
                    pl.when(has_guest)(lambda: back_copy(slot, guest).start())

    def square_copy(r, k, peer):
        return pltpu.make_async_remote_copy(
            src_ref=sq_send.at[r], dst_ref=sq_recv.at[r, k - 1], send_sem=sq_ss.at[r, k - 1],
            recv_sem=sq_rs.at[r, k - 1], device_id={"tp": peer}, device_id_type=MESH,
        )

    def squares_send(r):
        @pl.loop(0, seqs)
        def _(i):
            at = pl.ds(pl.multiple_of(r * rows + i * length, length), length)
            squares = jnp.sum(sq_acc[at, :], axis=1, keepdims=True)
            sq_send[r, i] = jnp.transpose(jnp.broadcast_to(squares, (length, length)))[:8, :]

        for k in range(1, n_tp):
            square_copy(r, k, lax.rem(t + k, n_tp)).start()

    def squares_total(r):
        for k in range(1, n_tp):
            square_copy(r, k, lax.rem(t + n_tp - k, n_tp)).wait_recv()
        total = sq_send[r]
        for k in range(1, n_tp):
            total = total + sq_recv[r, k - 1]
        return total

    def close(values, squares_of):
        gain = out_gain[:, own_columns(t)]

        @pl.loop(0, seqs)
        def _(i):
            factor = column(lax.rsqrt(squares_of[i][:1, :] / width + 1e-06))
            inside = pl.ds(pl.multiple_of(i * length, length), length)
            out_ref[inside, :] = (values[inside, :].astype(F32) * factor * gain).astype(BF16)

    def squares_back(device):
        return pltpu.make_async_remote_copy(
            src_ref=sq_back, dst_ref=sq_back, send_sem=guest_sem.at[2], recv_sem=guest_sem.at[3],
            device_id={"fs": device}, device_id_type=MESH,
        )

    guest = lax.select(f == 1, 0, n - 1)
    has_guest = (f == 1) | (f == n - 2)
    inward = lax.select(f == 0, 1, n - 2)

    def tokens_in(device):
        return pltpu.make_async_remote_copy(
            src_ref=tok_ref, dst_ref=block_of(tok_full, 1, t), send_sem=guest_sem.at[0], recv_sem=guest_sem.at[1],
            device_id={"fs": device}, device_id_type=MESH,
        )

    @pl.when(jnp.logical_not(is_host))
    def _():
        order = [("own", w, 0) for w in range(MIXER)] + [("tokens", 0, 0)]
        order += [("other", w, 0) for w in range(MIXER) if direct(w)]
        for c in range(counts[GATE]):
            order += [("own", GATE, c), ("own", UP, c), ("other", GATE, c), ("other", UP, c)]
        for kind in ("own", "other"):
            order += [(kind, DOWN, c) for c in range(pieces)]
        for kind, w, c in order:
            if kind == "own":
                start_own(w, c)
            elif kind == "tokens":
                tokens_in(inward).start()
            else:
                for k in range(1, parts):
                    other_half(w, c, k).start()
        tokens_in(inward).wait_send()
        for w in range(7):
            z_sent(w, f, lax.select(f == 0, 1, -1))
            if direct(w):
                for k in range(1, parts):
                    y_sent(w, f, k)
        for slot in range(columns // piece):
            back_copy(slot, inward).wait_recv()
        squares_back(inward).wait_recv()
        close(returned, sq_back)

    @pl.when(is_host)
    def _():
        own_tokens = pltpu.make_async_copy(tok_ref, block_of(tok_full, 0, t), own_sem.at[7])
        own_tokens.start()
        for w in range(MIXER):
            start_own(w, 0)
        for w in range(7):
            own_copy(w).start()
        own_tokens.wait()
        gather_send(tok_full, 0, 0)
        sq_acc[...] = jnp.zeros_like(sq_acc)
        for w in range(MIXER):
            from_inner(w, 0)
            from_outer(w, 0)
        last = counts[GATE] - 1

        def start_pair(c):
            if c <= last:
                start_own(GATE, c)
                start_own(UP, c)

        def inner_pair(c):
            if c <= last:
                from_inner(GATE, c)
                from_inner(UP, c)

        def outer_pair(c):
            if c <= last:
                from_outer(GATE, c)
                from_outer(UP, c)

        def far_pair(c):
            if c <= last:
                from_far(GATE, c)
                from_far(UP, c)

        def start_down(first, end):
            for c in range(first, min(end, pieces)):
                start_own(DOWN, c)

        def inner_down(c):
            if c < pieces:
                from_inner(DOWN, c)

        def outer_down(c):
            if c < pieces:
                from_outer(DOWN, c)

        def tile(c, r):
            if c <= last:
                if r == 0:
                    for w in (GATE, UP):
                        finish_all(w, c)
                hidden_tiles(c, r)

        def drain(group):
            for w in group:
                @pl.loop(0, n)
                def _(blk):
                    pl.when((f + 1 <= last_host) & (blk <= f))(lambda: z_sent(w, blk, 1))
                    pl.when((f - 1 >= first_host) & (blk >= f))(lambda: z_sent(w, blk, -1))
                    whole = ((blk == 0) & (f == 1)) | ((blk == n - 1) & (f == n - 2))
                    relayed = (blk != f) & jnp.logical_not(whole) if direct(w) else blk != f

                    @pl.when(relayed)
                    def _():
                        for k in range(1, parts):
                            y_sent(w, blk, k)

        start_pair(0)
        start_pair(1)
        gather_relay(tok_full, 0, 0)
        from_far(0, 0)
        gather_finish(tok_full, 0, 0)
        norm_rows(tok_full, mix_gain, 0)
        for w in range(1, MIXER):
            from_far(w, 0)

        @pl.when(has_guest)
        def _():
            tokens_in(guest).wait_recv()

        gather_send(tok_full, 0, 1)
        inner_pair(0)
        outer_pair(0)
        start_pair(2)
        for w in range(MIXER):
            own_copy(w).wait()
            finish_all(w, 0)
        mixer(0)
        sum_send(0)
        inner_pair(1)
        gather_relay(tok_full, 0, 1)
        sum_relay(0)
        gather_finish(tok_full, 0, 1)
        norm_rows(tok_full, mix_gain, 1)
        far_pair(0)
        mixer(1)
        sum_send(1)
        outer_pair(1)
        start_pair(3)
        sum_relay(1)
        inner_pair(2)
        first_rows(0)
        gather_send(first_full, 2, 0)
        far_pair(1)
        outer_pair(2)
        start_pair(4)
        inner_pair(3)
        first_rows(1)
        gather_send(first_full, 2, 1)
        far_pair(2)
        outer_pair(3)
        start_pair(5)
        inner_pair(4)
        for w in (GATE, UP):
            own_copy(w).wait()
        gather_relay(first_full, 2, 0)
        far_pair(3)
        gather_finish(first_full, 2, 0)
        norm_rows(first_full, ffn_gain, 0)
        outer_pair(4)
        start_down(0, 2)
        inner_pair(5)
        tile(0, 0)
        tile(1, 0)
        tile(2, 0)
        gather_relay(first_full, 2, 1)
        far_pair(4)
        outer_pair(5)
        start_down(2, pieces)
        gather_finish(first_full, 2, 1)
        norm_rows(first_full, ffn_gain, 1)
        for r in range(2):
            for k in range(chips):
                to_pair(r, k).wait_send()
            for k in range(1, chips):
                to_far(r, k).wait_send()
        tile(3, 0)
        inner_down(0)
        far_pair(5)
        tile(0, 1)
        outer_down(0)
        tile(1, 1)
        inner_down(1)
        tile(2, 1)
        outer_down(1)
        tile(3, 1)
        inner_down(2)
        tile(4, 0)
        tile(4, 1)
        outer_down(2)
        inner_down(3)
        tile(5, 0)
        tile(5, 1)
        for c in range(6, last + 1):
            start_pair(c)
            inner_pair(c)
            outer_pair(c)
            far_pair(c)
            tile(c, 0)
            tile(c, 1)
        for c in range(4, pieces):
            inner_down(c)
        own_copy(DOWN).wait()
        near = f + inner
        down_product(f, 0, wide)
        for c in range(pieces):
            to_lane(f, c)
        for c in range(3, pieces):
            outer_down(c)
        from_far(DOWN, 0)
        for c in range(pieces):
            finish(DOWN, c, near)
        down_product(near, 0, wide)
        for c in range(pieces):
            to_lane(near, c)
        for c in range(1, min(2, pieces)):
            from_far(DOWN, c)
        for c in range(pieces):
            combine(f, c)
        for c in range(2, min(3, pieces)):
            from_far(DOWN, c)
        for c in range(pieces):
            combine(near, c)
        drain(range(DOWN))
        for r in range(2):
            gather_sent(tok_full, 0, r)
            gather_sent(first_full, 2, r)
        for c in range(3, pieces):
            from_far(DOWN, c)

        def others(visit):
            @pl.loop(1, n - 2)
            def _(s):
                for toward in (inner, -inner):
                    b = f + toward * (1 + s)
                    pl.when((b >= 0) & (b < n))(lambda: visit(b))

        outer = f - inner

        def take(b, c):
            finish(DOWN, c, b)
            down_product(b, pl.multiple_of(c * piece, 128), piece)
            to_lane(b, c)

        @pl.loop(0, pieces)
        def _(c):
            others(lambda b: take(b, c))
            take(outer, c)
            others(lambda b: combine(b, c))
            combine(outer, c)

            @pl.when(c >= LAG)
            def _():
                others(lambda b: settle(b, c - LAG))
                settle(outer, c - LAG)

        @pl.loop(0, pieces)
        def _(i):
            settle(f, i)
            settle(near, i)

        for c in range(max(pieces - LAG, 0), pieces):
            others(lambda b: settle(b, c))
            settle(outer, c)

        squares_send(1)
        squares_send(0)
        sq_back[...] = squares_total(1)

        @pl.when(has_guest)
        def _():
            squares_back(guest).start()

        sq_total[...] = squares_total(0)
        close(second_own, sq_total)

        @pl.when(has_guest)
        def _():
            squares_back(guest).wait_send()
            back_sent()

        for r in range(2):
            for k in range(1, n_tp):
                square_copy(r, k, lax.rem(t + k, n_tp)).wait_send()
            for k in range(chips):
                down_sent(r, k)
        drain((DOWN,))


def solution(mesh):
    n, parts, n_tp = mesh.shape["fs"], mesh.shape["grp"], mesh.shape["tp"]

    def local(tokens, mix_gain, outer, inner, value, taps, mix_out, ffn_gain, gate, up, down, out_gain):
        seqs, length, columns = tokens.shape
        rows, width = seqs * length, columns * n_tp
        weights = (outer, inner, value, mix_out, gate, up, down)
        piece = min(down.shape[1], columns, 128)
        spans = [((0, a.shape[1]),) for a in weights]
        spans[GATE] = spans[UP] = tiles_of(gate.shape[1])
        spans[DOWN] = tuple((start, piece) for start in range(0, down.shape[1], piece))
        slots = sum(len(tiles) for tiles in spans)
        channels, units = outer.shape[1], gate.shape[1]
        others, y_others = max(n_tp - 1, 1), max(parts - 1, 1)
        per_owner = columns // piece
        dma = pltpu.SemaphoreType.DMA
        scratch = [pltpu.VMEM((n,) + a.shape, BF16) for a in weights]
        chips = n_tp // 2
        scratch += [
            pltpu.VMEM((2 * rows, width), BF16),
            pltpu.VMEM((2 * rows, width), BF16),
            pltpu.VMEM((3, rows, channels), BF16),
            pltpu.VMEM((rows, channels), BF16),
            pltpu.VMEM((2 * rows, width), BF16),
            pltpu.VMEM((2, chips, rows, columns), BF16),
            pltpu.VMEM((2, chips, rows, columns), BF16),
            pltpu.VMEM((2 * rows, width), BF16),
            pltpu.VMEM((2 * rows, units), BF16),
            pltpu.VMEM((rows, columns), BF16),
            pltpu.VMEM((rows, columns), F32),
            pltpu.VMEM((2 * rows, 128), F32),
            pltpu.VMEM((2, seqs, 8, length), F32),
            pltpu.VMEM((2, others, seqs, 8, length), F32),
            pltpu.VMEM((seqs, 8, length), F32),
            pltpu.VMEM((seqs, 8, length), F32),
            dma((7, n + 1)), dma((slots, n)),
            dma((7, n, y_others)), dma((slots, n, y_others)),
            dma((8,)), dma((3, 2, chips)), dma((3, 2, chips)), dma((3, 2, chips)), dma((3, 2, chips)),
            dma((2, chips)), dma((2, chips, per_owner)), dma((2, chips)), dma((2, chips, per_owner)),
            dma((2, others)), dma((2, others)), dma((1,)), dma((per_owner,)), dma((4,)),
        ]
        hbm, vmem = pl.BlockSpec(memory_space=pl.ANY), pl.BlockSpec(memory_space=pltpu.VMEM)
        out = pl.pallas_call(
            functools.partial(kernel, n, parts, n_tp, length, tuple(spans)),
            out_shape=jax.ShapeDtypeStruct((rows, columns), BF16),
            in_specs=[hbm, vmem, hbm, hbm, hbm, vmem, hbm, vmem, hbm, hbm, hbm, vmem],
            out_specs=pl.BlockSpec(memory_space=pltpu.VMEM),
            scratch_shapes=scratch,
            compiler_params=pltpu.CompilerParams(
                collective_id=0, has_side_effects=True, vmem_limit_bytes=62 * 1024 * 1024
            ),
        )(
            tokens.reshape(rows, columns), mix_gain[None], outer, inner, value, taps, mix_out,
            ffn_gain[None], gate, up, down, out_gain[None],
        )
        return out.reshape(seqs, length, columns)

    in_specs = (
        P(("grp", "fs"), None, "tp"), P(), P("fs", "tp"), P("fs", "tp"), P("fs", "tp"), P(), P("tp", "fs"),
        P(), P("fs", "tp"), P("fs", "tp"), P("tp", "fs"), P(),
    )
    out_specs = P(("grp", "fs"), None, "tp")
    return jax.shard_map(local, mesh=mesh, in_specs=in_specs, out_specs=out_specs, check_vma=False)
```

```python
import functools

import jax
import jax.numpy as jnp
from jax import lax
from jax.experimental import pallas as pl
from jax.experimental.pallas import tpu as pltpu
from jax.sharding import PartitionSpec as P

MESH = pl.DeviceIdType.MESH
F32 = jnp.float32
BF16 = jnp.bfloat16
MIXER = 4
GATE, UP, DOWN = 4, 5, 6
SHARED = 1
LAG = 2


def tiles_of(units):
    if units % 128:
        return ((0, units),)
    return tuple((start, min(256, units - start)) for start in range(0, units, 256))


def column(rows):
    wide = jnp.broadcast_to(rows, (rows.shape[1], rows.shape[1]))
    return jnp.transpose(wide)[:, :1]


def kernel(
    n, parts, n_tp, length, spans,
    tok_ref, mix_gain_in, w0, w1, w2, taps_in, w3, ffn_gain_in, w4, w5, w6, out_gain_in,
    out_ref,
    f0, f1, f2, f3, f4, f5, f6,
    tok_full, normed, proj, gated, part, pair_recv, far_recv, first_full, hidden, returned, second_own, sq_acc,
    sq_send, sq_recv, sq_total, mix_gain, taps_ref, ffn_gain, out_gain,
    z_send, z_recv, y_send, y_recv, own_sem, pair_ss, pair_rs, far_ss, far_rs,
    down_pair_ss, down_pair_rs, down_far_ss, down_far_rs, sq_ss, sq_rs, back_ss, back_rs, guest_sem,
):
    own = (w0, w1, w2, w3, w4, w5, w6)
    full = (f0, f1, f2, f3, f4, f5, f6)
    f, g, t = lax.axis_index("fs"), lax.axis_index("grp"), lax.axis_index("tp")
    rows, columns = tok_ref.shape
    width = columns * n_tp
    seqs = rows // length
    counts = [len(tiles) for tiles in spans]
    bases = [sum(counts[:w]) for w in range(7)]

    def y_peer(k):
        return lax.rem(g + k, parts)

    def tp_peer(k):
        return lax.rem(t + k, n_tp)

    def span(w, half, c):
        size = own[w].shape[0] // parts
        if isinstance(c, int):
            at = pl.ds(*spans[w][c])
        else:
            width_c = spans[w][0][1]
            at = pl.ds(pl.multiple_of(c * width_c, 128), width_c)
        return pl.ds(pl.multiple_of(half * size, 8), size), at

    def region(w, blk, half, c):
        at_rows, at_cols = span(w, half, c)
        return full[w].at[blk, at_rows, at_cols]

    def piece_of(w, half, c):
        at_rows, at_cols = span(w, half, c)
        return own[w].at[at_rows, at_cols]

    barrier = pltpu.get_barrier_semaphore()
    for k in range(1, n_tp):
        pl.semaphore_signal(barrier, inc=1, device_id={"tp": tp_peer(k)}, device_id_type=MESH)
    for k in range(1, parts):
        pl.semaphore_signal(barrier, inc=1, device_id={"grp": y_peer(k)}, device_id_type=MESH)

    @pl.when(f < n - 1)
    def _():
        pl.semaphore_signal(barrier, inc=1, device_id={"fs": f + 1}, device_id_type=MESH)

    @pl.when(f > 0)
    def _():
        pl.semaphore_signal(barrier, inc=1, device_id={"fs": f - 1}, device_id_type=MESH)

    neighbours = lax.min(f, 1) + lax.min(n - 1 - f, 1)
    pl.semaphore_wait(barrier, n_tp - 1 + parts - 1 + neighbours)

    def z_slot(blk, step):
        return lax.select((blk == f) & (step < 0), n, blk)

    def half_block(w, blk):
        size = own[w].shape[0] // parts
        return full[w].at[blk, pl.ds(pl.multiple_of(g * size, 8), size), :]

    def z_sent(w, blk, step):
        half = half_block(w, blk)
        pltpu.make_async_remote_copy(
            src_ref=half, dst_ref=half, send_sem=z_send.at[w, z_slot(blk, step)], recv_sem=z_recv.at[bases[w], blk],
            device_id={"fs": f + step}, device_id_type=MESH,
        ).wait_send()

    def y_sent(w, blk, k):
        half = half_block(w, blk)
        pltpu.make_async_remote_copy(
            src_ref=half, dst_ref=half, send_sem=y_send.at[w, blk, k - 1], recv_sem=y_recv.at[bases[w], blk, k - 1],
            device_id={"grp": y_peer(k)}, device_id_type=MESH,
        ).wait_send()

    def z_copy(w, c, blk, src, step):
        return pltpu.make_async_remote_copy(
            src_ref=src, dst_ref=region(w, blk, g, c),
            send_sem=z_send.at[w, z_slot(blk, step)], recv_sem=z_recv.at[bases[w] + c, blk],
            device_id={"fs": f + step}, device_id_type=MESH,
        )

    def y_copy(w, c, blk, half, k, peer):
        return pltpu.make_async_remote_copy(
            src_ref=region(w, blk, half, c), dst_ref=region(w, blk, half, c),
            send_sem=y_send.at[w, blk, k - 1], recv_sem=y_recv.at[bases[w] + c, blk, k - 1],
            device_id={"grp": peer}, device_id_type=MESH,
        )

    first_host, last_host = 1, n - 2
    is_host = (f >= first_host) & (f <= last_host)
    inner = lax.select(2 * f + 1 < n, 1, -1)

    def start_own(w, c):
        src = piece_of(w, g, c)

        @pl.when(f + 1 <= last_host)
        def _():
            z_copy(w, c, f, src, 1).start()

        @pl.when(f - 1 >= first_host)
        def _():
            z_copy(w, c, f, src, -1).start()

    def other_half(w, c, k):
        half = lax.rem(g + parts - k, parts)
        inward = lax.select(f == 0, 1, n - 2)
        return pltpu.make_async_remote_copy(
            src_ref=piece_of(w, half, c), dst_ref=region(w, f, half, c),
            send_sem=y_send.at[w, f, k - 1], recv_sem=y_recv.at[bases[w] + c, f, k - 1],
            device_id={"fs": inward}, device_id_type=MESH,
        )

    def direct(w):
        return w >= SHARED

    def relay(w, c, s, toward, next_to_edge):
        blk = f + toward * (1 + s)
        step = -toward

        @pl.when((blk >= 0) & (blk < n))
        def _():
            z_copy(w, c, blk, region(w, blk, g, c), step).wait_recv()

            def share():
                for k in range(1, parts):
                    y_copy(w, c, blk, g, k, y_peer(k)).start()

            def onward():
                z_copy(w, c, blk, region(w, blk, g, c), step).start()

            pl.when((f + step <= last_host) & (f + step >= first_host))(onward)
            if next_to_edge and direct(w):
                pl.when((blk > 0) & (blk < n - 1))(share)
            else:
                share()

    def from_inner(w, c):
        relay(w, c, 0, inner, True)

    def from_outer(w, c):
        relay(w, c, 0, -inner, True)

    def from_far(w, c):
        @pl.loop(1, n - 2)
        def _(s):
            relay(w, c, s, inner, False)
            relay(w, c, s, -inner, False)

    def finish(w, c, blk):
        for k in range(1, parts):
            source = lax.rem(g + parts - k, parts)
            y_copy(w, c, blk, source, k, source).wait_recv()

    def finish_all(w, c):
        @pl.loop(0, n)
        def _(blk):
            pl.when(blk != f)(lambda: finish(w, c, blk))

    def own_copy(w):
        return pltpu.make_async_copy(own[w], full[w].at[f], own_sem.at[w])

    def small_copy(i):
        pairs = ((mix_gain_in, mix_gain), (taps_in, taps_ref), (ffn_gain_in, ffn_gain), (out_gain_in, out_gain))
        return pltpu.make_async_copy(*pairs[i], own_sem.at[8 + i])

    def own_columns(owner):
        return pl.ds(pl.multiple_of(owner * columns, 128), columns)

    chips = n_tp // 2
    core = lax.rem(t, 2)
    pair = t + 1 - 2 * core

    def ahead(k, start=None):
        return lax.rem((t if start is None else start) + 2 * k, n_tp)

    def behind(k, start=None):
        return lax.rem((t if start is None else start) + n_tp - 2 * k, n_tp)

    def set_rows(r):
        return pl.ds(r * rows, rows)

    def pair_copy(stage, r, k, src, dst):
        return pltpu.make_async_remote_copy(
            src_ref=src, dst_ref=dst, send_sem=pair_ss.at[stage, r, k], recv_sem=pair_rs.at[stage, r, k],
            device_id={"tp": pair}, device_id_type=MESH,
        )

    def far_copy(stage, r, k, src, dst, peer):
        return pltpu.make_async_remote_copy(
            src_ref=src, dst_ref=dst, send_sem=far_ss.at[stage, r, k], recv_sem=far_rs.at[stage, r, k],
            device_id={"tp": peer}, device_id_type=MESH,
        )

    def block_of(buf, r, owner):
        return buf.at[set_rows(r), own_columns(owner)]

    def gather_send(buf, stage, r):
        mine = block_of(buf, r, t)
        for k in range(1, chips):
            far_copy(stage, r, k, mine, mine, ahead(k)).start()
        pair_copy(stage, r, 0, mine, mine).start()

    def gather_relay(buf, stage, r):
        for k in range(1, chips):
            theirs = block_of(buf, r, behind(k))
            far_copy(stage, r, k, theirs, theirs, behind(k)).wait_recv()
            pair_copy(stage, r, k, theirs, theirs).start()

    def gather_finish(buf, stage, r):
        for k in range(chips):
            theirs = block_of(buf, r, behind(k, pair))
            pair_copy(stage, r, k, theirs, theirs).wait_recv()

    def gather_sent(buf, stage, r):
        mine = block_of(buf, r, t)
        for k in range(1, chips):
            far_copy(stage, r, k, mine, mine, ahead(k)).wait_send()
        for k in range(chips):
            pair_copy(stage, r, k, mine, mine).wait_send()

    def to_pair(r, k):
        return pair_copy(1, r, k, block_of(part, r, ahead(k, pair)), pair_recv.at[r, k])

    def to_far(r, k):
        return far_copy(1, r, k, block_of(part, r, ahead(k)), far_recv.at[r, k], ahead(k))

    def sum_send(r):
        for k in range(chips - 1, -1, -1):
            to_pair(r, k).start()

    def sum_relay(r):
        for k in range(1, chips):
            to_pair(r, k).wait_recv()

            @pl.loop(0, rows // 64)
            def _(i):
                inside = pl.ds(pl.multiple_of(i * 64, 64), 64)
                at = pl.ds(pl.multiple_of(r * rows + i * 64, 64), 64)
                both = part[at, own_columns(ahead(k))].astype(F32) + pair_recv[r, k, inside, :].astype(F32)
                part[at, own_columns(ahead(k))] = both.astype(BF16)

            to_far(r, k).start()

    def summed(r, start, size):
        inside = pl.ds(pl.multiple_of(start, size), size)
        at = pl.ds(pl.multiple_of(r * rows + start, size), size)
        total = part[at, own_columns(t)].astype(F32) + pair_recv[r, 0, inside, :].astype(F32)
        for k in range(1, chips):
            total = total + far_recv[r, k, inside, :].astype(F32)
        return at, total

    def first_rows(r):
        to_pair(r, 0).wait_recv()
        for k in range(1, chips):
            to_far(r, k).wait_recv()

        @pl.loop(0, rows // 64)
        def _(i):
            at, total = summed(r, i * 64, 64)
            first_full[at, own_columns(t)] = (tok_full[at, own_columns(t)].astype(F32) + total).astype(BF16)

    def norm_rows(source, gain, r):
        size = 32

        @pl.loop(0, rows // size)
        def _(i):
            at = pl.ds(pl.multiple_of(r * rows + i * size, size), size)
            values = source[at, :].astype(F32)
            scale = lax.rsqrt(jnp.sum(values * values, axis=1, keepdims=True) / width + 1e-06)
            normed[at, :] = (values * scale * gain[...]).astype(BF16)

    channels = w0.shape[1]
    block = w3.shape[1]
    units = w4.shape[1]
    tap_count = taps_ref.shape[0]

    def project(w, r):
        weight = full[w][...].reshape(width, channels)
        proj[w] = jnp.dot(normed[set_rows(r), :], weight, preferred_element_type=F32).astype(BF16)

    def convolve():
        taps = taps_ref[:, pl.ds(pl.multiple_of(t * channels, 128), channels)]

        @pl.loop(0, seqs)
        def _(i):
            at = pl.ds(pl.multiple_of(i * length, length), length)
            product = proj[1, at, :].astype(F32) * proj[2, at, :].astype(F32)
            position = lax.broadcasted_iota(jnp.int32, product.shape, 0)
            conv = jnp.zeros_like(product)
            for offset in range(tap_count):
                shift = tap_count - 1 - offset
                moved = product if shift == 0 else jnp.where(position >= shift, pltpu.roll(product, shift, 0), 0.0)
                conv = conv + taps[offset : offset + 1, :] * moved
            gated[at, :] = (proj[0, at, :].astype(F32) * conv).astype(BF16)

    def mix(r):
        @pl.loop(0, n)
        def _(b):
            at = pl.ds(pl.multiple_of(b * block, 128), block)
            part[set_rows(r), at] = jnp.dot(gated[...], full[3][b], preferred_element_type=F32).astype(BF16)

    def hidden_tile(r, start, size):
        at = pl.ds(start, size)
        left = normed[set_rows(r), :]
        gate = jnp.dot(left, full[GATE][:, :, at].reshape(width, size), preferred_element_type=F32)
        upward = jnp.dot(left, full[UP][:, :, at].reshape(width, size), preferred_element_type=F32)
        hidden[set_rows(r), at] = (gate / (1.0 + jnp.exp(-gate)) * upward).astype(BF16)

    def hidden_tiles(c, r):
        first, total = spans[GATE][c]
        for offset in range(0, total, 256):
            hidden_tile(r, first + offset, min(256, total - offset))

    wide = w6.shape[1]
    piece = spans[DOWN][0][1]
    pieces = counts[DOWN]

    def down_to_pair(r, k, slot, start):
        inside = pl.ds(pl.multiple_of(slot * piece, 128), piece)
        return pltpu.make_async_remote_copy(
            src_ref=part.at[set_rows(r), pl.ds(start, piece)], dst_ref=pair_recv.at[r, k, :, inside],
            send_sem=down_pair_ss.at[r, k], recv_sem=down_pair_rs.at[r, k, slot],
            device_id={"tp": pair}, device_id_type=MESH,
        )

    def down_to_far(r, k, slot, start):
        inside = pl.ds(pl.multiple_of(slot * piece, 128), piece)
        return pltpu.make_async_remote_copy(
            src_ref=part.at[set_rows(r), pl.ds(start, piece)], dst_ref=far_recv.at[r, k, :, inside],
            send_sem=down_far_ss.at[r, k], recv_sem=down_far_rs.at[r, k, slot],
            device_id={"tp": lax.rem(t + 2 * k, n_tp)}, device_id_type=MESH,
        )

    def down_sent(r, k):
        whole = pair_recv.at[r, k]
        pltpu.make_async_remote_copy(
            src_ref=whole, dst_ref=whole, send_sem=down_pair_ss.at[r, k], recv_sem=down_pair_rs.at[r, k, 0],
            device_id={"tp": pair}, device_id_type=MESH,
        ).wait_send()
        if k > 0:
            pltpu.make_async_remote_copy(
                src_ref=whole, dst_ref=whole, send_sem=down_far_ss.at[r, k], recv_sem=down_far_rs.at[r, k, 0],
                device_id={"tp": lax.rem(t + 2 * k, n_tp)}, device_id_type=MESH,
            ).wait_send()

    def place(b, c):
        start = pl.multiple_of(b * wide + c * piece, 128)
        owner = (b * wide + c * piece) // columns
        slot = lax.rem(b * wide + c * piece, columns) // piece
        k = lax.rem(owner // 2 - t // 2 + chips, chips)
        return start, owner, slot, k, lax.rem(owner, 2) == core

    def down_product(b, r, offset, size):
        weight = full[DOWN][b, :, pl.ds(offset, size)]
        part[set_rows(r), pl.ds(pl.multiple_of(b * wide + offset, 128), size)] = jnp.dot(
            hidden[set_rows(r), :], weight, preferred_element_type=F32
        ).astype(BF16)

    def to_lane(b, c):
        start, owner, slot, k, lane = place(b, c)

        @pl.when(jnp.logical_not(lane))
        def _():
            for r in (1, 0):
                down_to_pair(r, k, slot, start).start()

    def combine(b, c):
        start, owner, slot, k, lane = place(b, c)

        @pl.when(lane & (k > 0))
        def _():
            inside = pl.ds(pl.multiple_of(slot * piece, 128), piece)
            for r in (1, 0):
                down_to_pair(r, k, slot, start).wait_recv()

                @pl.loop(0, rows // 64)
                def _(i):
                    here = pl.ds(pl.multiple_of(i * 64, 64), 64)
                    at = pl.ds(pl.multiple_of(r * rows + i * 64, 64), 64)
                    both = part[at, pl.ds(start, piece)].astype(F32) + pair_recv[r, k, here, inside].astype(F32)
                    part[at, pl.ds(start, piece)] = both.astype(BF16)

                down_to_far(r, k, slot, start).start()

    def back_copy(slot, device):
        at = pl.ds(pl.multiple_of(slot * piece, 128), piece)
        return pltpu.make_async_remote_copy(
            src_ref=returned.at[:, at], dst_ref=returned.at[:, at], send_sem=back_ss.at[0], recv_sem=back_rs.at[slot],
            device_id={"fs": device}, device_id_type=MESH,
        )

    def back_sent():
        pltpu.make_async_remote_copy(
            src_ref=returned, dst_ref=returned, send_sem=back_ss.at[0], recv_sem=back_rs.at[0],
            device_id={"fs": guest}, device_id_type=MESH,
        ).wait_send()

    def settle(b, c):
        start, owner, slot, k, lane = place(b, c)

        @pl.when(owner == t)
        def _():
            inside = pl.ds(pl.multiple_of(slot * piece, 128), piece)
            for r in (1, 0):
                down_to_pair(r, 0, slot, start).wait_recv()
                for far in range(1, chips):
                    down_to_far(r, far, slot, start).wait_recv()

                @pl.loop(0, rows // 64)
                def _(i):
                    here = pl.ds(pl.multiple_of(i * 64, 64), 64)
                    at = pl.ds(pl.multiple_of(r * rows + i * 64, 64), 64)
                    total = part[at, pl.ds(start, piece)].astype(F32) + pair_recv[r, 0, here, inside].astype(F32)
                    for far in range(1, chips):
                        total = total + far_recv[r, far, here, inside].astype(F32)
                    second = first_full[at, pl.ds(start, piece)].astype(F32) + total
                    squares = second * second
                    folded = squares[:, :128]
                    for lane_block in range(1, piece // 128):
                        folded = folded + squares[:, lane_block * 128 : (lane_block + 1) * 128]
                    sq_acc[at, :] += folded
                    if r == 0:
                        second_own[here, inside] = second
                    else:
                        returned[here, inside] = second.astype(BF16)

                if r == 1:
                    pl.when(has_guest)(lambda: back_copy(slot, guest).start())

    guest = lax.select(f == 1, 0, n - 1)

    def ahead_of(k):
        return lax.rem(t + k, n_tp)

    def square_copy(k, peer):
        return pltpu.make_async_remote_copy(
            src_ref=sq_send.at[0], dst_ref=sq_recv.at[0, k], send_sem=sq_ss.at[0, k],
            recv_sem=sq_rs.at[0, k], device_id={"tp": peer}, device_id_type=MESH,
        )

    def edge_squares(k, peer):
        return pltpu.make_async_remote_copy(
            src_ref=sq_send.at[1], dst_ref=sq_recv.at[1, k], send_sem=sq_ss.at[1, k],
            recv_sem=sq_rs.at[1, k], device_id={"fs": guest, "tp": peer}, device_id_type=MESH,
        )

    def squares_of(r):
        @pl.loop(0, seqs)
        def _(i):
            at = pl.ds(pl.multiple_of(r * rows + i * length, length), length)
            squares = jnp.sum(sq_acc[at, :], axis=1, keepdims=True)
            sq_send[r, i] = jnp.transpose(jnp.broadcast_to(squares, (length, length)))[:8, :]

    def squares_total():
        total = sq_send[0]
        for k in range(1, n_tp):
            square_copy(k, t).wait_recv()
            total = total + sq_recv[0, k]
        return total

    def close(values, squares):
        gain = out_gain[:, own_columns(t)]

        @pl.loop(0, seqs)
        def _(i):
            factor = column(lax.rsqrt(squares[i][:1, :] / width + 1e-06))
            inside = pl.ds(pl.multiple_of(i * length, length), length)
            out_ref[inside, :] = (values[inside, :].astype(F32) * factor * gain).astype(BF16)

    has_guest = (f == 1) | (f == n - 2)
    inward = lax.select(f == 0, 1, n - 2)

    def tokens_in(device):
        return pltpu.make_async_remote_copy(
            src_ref=tok_ref, dst_ref=block_of(tok_full, 1, t), send_sem=guest_sem.at[0], recv_sem=guest_sem.at[1],
            device_id={"fs": device}, device_id_type=MESH,
        )

    @pl.when(jnp.logical_not(is_host))
    def _():
        small_copy(3).start()
        small_copy(3).wait()
        order = [("own", w, 0) for w in range(MIXER)] + [("tokens", 0, 0)]
        order += [("other", w, 0) for w in range(MIXER) if direct(w)]
        for c in range(counts[GATE] + 1):
            order += [("own", w, c) for w in (GATE, UP) if c < counts[GATE]]
            order += [("other", w, c - 1) for w in (GATE, UP) if c > 0]
        for kind in ("own", "other"):
            order += [(kind, DOWN, c) for c in range(pieces)]
        for kind, w, c in order:
            if kind == "own":
                start_own(w, c)
            elif kind == "tokens":
                tokens_in(inward).start()
            else:
                for k in range(1, parts):
                    other_half(w, c, k).start()
        tokens_in(inward).wait_send()
        for w in range(7):
            z_sent(w, f, lax.select(f == 0, 1, -1))
            if direct(w):
                for k in range(1, parts):
                    y_sent(w, f, k)
        for slot in range(columns // piece):
            back_copy(slot, inward).wait_recv()
        for k in range(n_tp):
            edge_squares(k, t).wait_recv()
        sq_total[...] = sum(sq_recv[1, k] for k in range(1, n_tp)) + sq_recv[1, 0]
        close(returned, sq_total)

    @pl.when(is_host)
    def _():
        own_tokens = pltpu.make_async_copy(tok_ref, block_of(tok_full, 0, t), own_sem.at[7])
        own_tokens.start()
        for w in range(MIXER):
            start_own(w, 0)
        for i in range(4):
            small_copy(i).start()
        for w in range(7):
            own_copy(w).start()
        own_tokens.wait()
        gather_send(tok_full, 0, 0)
        for i in range(4):
            small_copy(i).wait()
        sq_acc[...] = jnp.zeros_like(sq_acc)
        for w in range(MIXER):
            from_inner(w, 0)
            from_outer(w, 0)
        last = counts[GATE] - 1

        def start_pair(c):
            if c <= last:
                start_own(GATE, c)
                start_own(UP, c)

        def inner_pair(c):
            if c <= last:
                from_inner(GATE, c)
                from_inner(UP, c)

        def outer_pair(c):
            if c <= last:
                from_outer(GATE, c)
                from_outer(UP, c)

        def far_pair(c):
            if c <= last:
                from_far(GATE, c)
                from_far(UP, c)

        def start_down(first, end):
            for c in range(first, min(end, pieces)):
                start_own(DOWN, c)

        def inner_down(c):
            if c < pieces:
                from_inner(DOWN, c)

        def outer_down(c):
            if c < pieces:
                from_outer(DOWN, c)

        def tile(c, r):
            if c <= last:
                if r == 0:
                    for w in (GATE, UP):
                        finish_all(w, c)
                hidden_tiles(c, r)

        def drain(group):
            for w in group:
                @pl.loop(0, n)
                def _(blk):
                    pl.when((f + 1 <= last_host) & (blk <= f))(lambda: z_sent(w, blk, 1))
                    pl.when((f - 1 >= first_host) & (blk >= f))(lambda: z_sent(w, blk, -1))
                    whole = ((blk == 0) & (f == 1)) | ((blk == n - 1) & (f == n - 2))
                    relayed = (blk != f) & jnp.logical_not(whole) if direct(w) else blk != f

                    @pl.when(relayed)
                    def _():
                        for k in range(1, parts):
                            y_sent(w, blk, k)

        start_pair(0)
        start_pair(1)
        gather_relay(tok_full, 0, 0)
        from_far(0, 0)
        gather_finish(tok_full, 0, 0)
        norm_rows(tok_full, mix_gain, 0)
        for w in range(1, MIXER):
            from_far(w, 0)

        @pl.when(has_guest)
        def _():
            tokens_in(guest).wait_recv()

        gather_send(tok_full, 0, 1)
        inner_pair(0)
        for w in range(3):
            own_copy(w).wait()
            finish_all(w, 0)
            project(w, 0)
        outer_pair(0)
        start_pair(2)
        start_down(0, 1)
        convolve()
        own_copy(3).wait()
        finish_all(3, 0)
        mix(0)
        sum_send(0)
        gather_relay(tok_full, 0, 1)
        inner_pair(1)
        gather_finish(tok_full, 0, 1)
        sum_relay(0)
        norm_rows(tok_full, mix_gain, 1)
        far_pair(0)
        for w in range(3):
            project(w, 1)
        convolve()
        mix(1)
        sum_send(1)
        outer_pair(1)
        start_pair(3)
        sum_relay(1)
        inner_pair(2)
        first_rows(0)
        gather_send(first_full, 2, 0)
        outer_pair(2)
        start_pair(4)
        inner_down(0)
        far_pair(1)
        inner_pair(3)
        outer_pair(3)
        start_pair(5)
        start_down(1, 2)
        first_rows(1)
        gather_send(first_full, 2, 1)
        far_pair(2)
        gather_relay(first_full, 2, 0)
        outer_pair(4)
        inner_pair(4)
        for w in (GATE, UP):
            own_copy(w).wait()
        gather_finish(first_full, 2, 0)
        norm_rows(first_full, ffn_gain, 0)
        far_pair(3)
        tile(0, 0)
        outer_pair(5)
        start_down(2, pieces)
        inner_pair(5)
        inner_down(1)
        tile(1, 0)
        tile(2, 0)
        gather_relay(first_full, 2, 1)
        far_pair(4)
        gather_finish(first_full, 2, 1)
        norm_rows(first_full, ffn_gain, 1)
        far_pair(5)
        tile(3, 0)
        for r in range(2):
            for k in range(chips):
                to_pair(r, k).wait_send()
            for k in range(1, chips):
                to_far(r, k).wait_send()
        tile(0, 1)
        tile(1, 1)
        tile(2, 1)
        outer_down(0)
        tile(3, 1)
        inner_down(2)
        tile(4, 0)
        tile(4, 1)
        outer_down(1)
        tile(5, 0)
        inner_down(3)
        tile(5, 1)
        for c in range(6, last + 1):
            start_pair(c)
            inner_pair(c)
            outer_pair(c)
            far_pair(c)
            tile(c, 0)
            tile(c, 1)
        own_copy(DOWN).wait()
        near, outer = f + inner, f - inner
        batch = 2 if pieces % 2 == 0 else 1

        def produce(b, first, count):
            for r in (1, 0):
                down_product(b, r, pl.multiple_of(first * piece, 128), count * piece)
            for i in range(count):
                to_lane(b, first + i)

        def far_down(c):
            if c < pieces:
                from_far(DOWN, c)

        def near_pieces(first, count):
            for c in range(first, first + count):
                finish(DOWN, c, near)
            produce(near, first, count)

        near_pieces(0, batch)
        outer_down(2)
        produce(f, 0, pieces)
        far_down(0)
        for c in range(batch):
            combine(near, c)
        for c in range(3, pieces):
            outer_down(c)
        for c in range(pieces):
            combine(f, c)
        for first in range(batch, pieces, batch):
            near_pieces(first, batch)
        far_down(1)
        for c in range(batch, pieces):
            combine(near, c)
        far_down(2)
        drain(range(DOWN))
        for r in range(2):
            gather_sent(tok_full, 0, r)
            gather_sent(first_full, 2, r)

        def others(visit):
            @pl.loop(1, n - 2)
            def _(s):
                for toward in (inner, -inner):
                    b = f + toward * (1 + s)
                    pl.when((b >= 0) & (b < n))(lambda: visit(b))

        def take(b, first, count):
            for c in range(first, first + count):
                finish(DOWN, c, b)
            produce(b, first, count)

        def join(b, first, count):
            for c in range(first, first + count):
                combine(b, c)

        def settle_range(first, end):
            @pl.loop(first, end)
            def _(i):
                settle(f, i)
                settle(near, i)

        batches = [(0, batch)] + [(c, 1) for c in range(batch, pieces)]
        for first, count in batches:
            take(outer, first, count)
            for c in range(max(first + count, 3), pieces if first == 0 else 0):
                from_far(DOWN, c)
            if first + count == pieces:
                settle_range(pieces // 2, pieces)
            elif first > 0:
                settle_range(0, pieces // 2)
            others(lambda b: take(b, first, count))

            join(outer, first, count)
            others(lambda b: join(b, first, count))

        @pl.loop(0, pieces)
        def _(c):
            others(lambda b: settle(b, c))
            settle(outer, c)

        squares_of(1)

        @pl.when(has_guest)
        def _():
            for k in range(n_tp):
                edge_squares(k, ahead_of(k)).start()

        squares_of(0)
        for k in range(1, n_tp):
            square_copy(k, ahead_of(k)).start()
        sq_total[...] = squares_total()
        close(second_own, sq_total)

        @pl.when(has_guest)
        def _():
            for k in range(n_tp):
                edge_squares(k, ahead_of(k)).wait_send()
            back_sent()

        for k in range(1, n_tp):
            square_copy(k, ahead_of(k)).wait_send()
        for r in range(2):
            for k in range(chips):
                down_sent(r, k)
        drain((DOWN,))


def solution(mesh):
    n, parts, n_tp = mesh.shape["fs"], mesh.shape["grp"], mesh.shape["tp"]

    def local(tokens, mix_gain, outer, inner, value, taps, mix_out, ffn_gain, gate, up, down, out_gain):
        seqs, length, columns = tokens.shape
        rows, width = seqs * length, columns * n_tp
        weights = (outer, inner, value, mix_out, gate, up, down)
        piece = min(down.shape[1], columns, 128)
        spans = [((0, a.shape[1]),) for a in weights]
        spans[GATE] = spans[UP] = tiles_of(gate.shape[1])
        spans[DOWN] = tuple((start, piece) for start in range(0, down.shape[1], piece))
        slots = sum(len(tiles) for tiles in spans)
        channels, units = outer.shape[1], gate.shape[1]
        y_others = max(parts - 1, 1)
        per_owner = columns // piece
        dma = pltpu.SemaphoreType.DMA
        scratch = [pltpu.VMEM((n,) + a.shape, BF16) for a in weights]
        chips = n_tp // 2
        scratch += [
            pltpu.VMEM((2 * rows, width), BF16),
            pltpu.VMEM((2 * rows, width), BF16),
            pltpu.VMEM((3, rows, channels), BF16),
            pltpu.VMEM((rows, channels), BF16),
            pltpu.VMEM((2 * rows, width), BF16),
            pltpu.VMEM((2, chips, rows, columns), BF16),
            pltpu.VMEM((2, chips, rows, columns), BF16),
            pltpu.VMEM((2 * rows, width), BF16),
            pltpu.VMEM((2 * rows, units), BF16),
            pltpu.VMEM((rows, columns), BF16),
            pltpu.VMEM((rows, columns), F32),
            pltpu.VMEM((2 * rows, 128), F32),
            pltpu.VMEM((2, seqs, 8, length), F32),
            pltpu.VMEM((2, n_tp, seqs, 8, length), F32),
            pltpu.VMEM((seqs, 8, length), F32),
            pltpu.VMEM((1, width), F32), pltpu.VMEM(taps.shape, F32),
            pltpu.VMEM((1, width), F32), pltpu.VMEM((1, width), F32),
            dma((7, n + 1)), dma((slots, n)),
            dma((7, n, y_others)), dma((slots, n, y_others)),
            dma((12,)), dma((3, 2, chips)), dma((3, 2, chips)), dma((3, 2, chips)), dma((3, 2, chips)),
            dma((2, chips)), dma((2, chips, per_owner)), dma((2, chips)), dma((2, chips, per_owner)),
            dma((2, n_tp)), dma((2, n_tp)), dma((1,)), dma((per_owner,)), dma((2,)),
        ]
        out = pl.pallas_call(
            functools.partial(kernel, n, parts, n_tp, length, tuple(spans)),
            out_shape=jax.ShapeDtypeStruct((rows, columns), BF16),
            in_specs=[pl.BlockSpec(memory_space=pl.ANY)] * 12,
            out_specs=pl.BlockSpec(memory_space=pltpu.VMEM),
            scratch_shapes=scratch,
            compiler_params=pltpu.CompilerParams(
                collective_id=0, has_side_effects=True, vmem_limit_bytes=62 * 1024 * 1024
            ),
        )(
            tokens.reshape(rows, columns), mix_gain[None], outer, inner, value, taps, mix_out,
            ffn_gain[None], gate, up, down, out_gain[None],
        )
        return out.reshape(seqs, length, columns)

    in_specs = (
        P(("grp", "fs"), None, "tp"), P(), P("fs", "tp"), P("fs", "tp"), P("fs", "tp"), P(), P("tp", "fs"),
        P(), P("fs", "tp"), P("fs", "tp"), P("tp", "fs"), P(),
    )
    out_specs = P(("grp", "fs"), None, "tp")
    return jax.shard_map(local, mesh=mesh, in_specs=in_specs, out_specs=out_specs, check_vma=False)
```

```python
import functools

import jax
import jax.numpy as jnp
from jax import lax
from jax.experimental import pallas as pl
from jax.experimental.pallas import tpu as pltpu
from jax.sharding import PartitionSpec as P

MESH = pl.DeviceIdType.MESH
F32 = jnp.float32
BF16 = jnp.bfloat16
MIXER = 4
GATE, UP, DOWN = 4, 5, 6
SHARED = 1
TRAIL = 2
LAG = 2


def tiles_of(units):
    if units % 128:
        return ((0, units),)
    return tuple((start, min(256, units - start)) for start in range(0, units, 256))


def spread(rows):
    return jnp.transpose(jnp.broadcast_to(rows, (rows.shape[1], rows.shape[1])))


def kernel(
    n, parts, n_tp, length, spans,
    tok_ref, mix_gain_in, w0, w1, w2, taps_in, w3, ffn_gain_in, w4, w5, w6, out_gain_in,
    out_ref,
    f0, f1, f2, f3, pair_full, f6,
    tok_full, normed, proj, gated, part, pair_recv, far_recv, first_full, hidden, returned, second_own, sq_acc,
    sq_send, sq_recv, sq_total, mix_gain, taps_ref, ffn_gain, out_gain,
    z_send, z_recv, y_send, y_recv, own_sem, pair_ss, pair_rs, far_ss, far_rs,
    down_pair_ss, down_pair_rs, down_far_ss, down_far_rs, sq_ss, sq_rs, back_ss, back_rs, guest_sem,
):
    own = (w0, w1, w2, w3, w4, w5, w6)
    full = (f0, f1, f2, f3, pair_full.at[0], pair_full.at[1], f6)
    f, g, t = lax.axis_index("fs"), lax.axis_index("grp"), lax.axis_index("tp")
    rows, columns = tok_ref.shape
    width = columns * n_tp
    seqs = rows // length
    counts = [len(tiles) for tiles in spans]
    groups = (0, 1, 2, 3, GATE, DOWN)
    ranks = {w: i for i, w in enumerate(groups)}
    bases = {w: sum(counts[v] for v in groups[:i]) for w, i in ranks.items()}

    def y_peer(k):
        return lax.rem(g + k, parts)

    def tp_peer(k):
        return lax.rem(t + k, n_tp)

    def span(w, half, c):
        size = own[w].shape[0] // parts
        if isinstance(c, int):
            at = pl.ds(*spans[w][c])
        else:
            width_c = spans[w][0][1]
            at = pl.ds(pl.multiple_of(c * width_c, 128), width_c)
        return pl.ds(pl.multiple_of(half * size, 8), size), at

    def members(w):
        return (GATE, UP) if w == GATE else (w,)

    def region(w, blk, half, c):
        at_rows, at_cols = span(w, half, c)
        if w == GATE:
            return pair_full.at[:, blk, at_rows, at_cols]
        return full[w].at[blk, at_rows, at_cols]

    def landing(v, blk, half, c):
        at_rows, at_cols = span(v, half, c)
        if v in (GATE, UP):
            return pair_full.at[v - GATE, blk, at_rows, at_cols]
        return full[v].at[blk, at_rows, at_cols]

    def piece_of(w, half, c):
        at_rows, at_cols = span(w, half, c)
        return own[w].at[at_rows, at_cols]

    def small_copy(i):
        pairs = ((mix_gain_in, mix_gain), (taps_in, taps_ref), (ffn_gain_in, ffn_gain), (out_gain_in, out_gain))
        return pltpu.make_async_copy(*pairs[i], own_sem.at[8 + i])

    def own_tokens():
        mine = tok_full.at[pl.ds(0, rows), pl.ds(pl.multiple_of(t * columns, 128), columns)]
        return pltpu.make_async_copy(tok_ref, mine, own_sem.at[7])

    hosting = (f >= 1) & (f <= n - 2)
    small_copy(3).start()

    @pl.when(hosting)
    def _():
        own_tokens().start()
        for i in range(3):
            small_copy(i).start()

    barrier = pltpu.get_barrier_semaphore()
    for k in range(1, n_tp):
        pl.semaphore_signal(barrier, inc=1, device_id={"tp": tp_peer(k)}, device_id_type=MESH)
    for k in range(1, parts):
        pl.semaphore_signal(barrier, inc=1, device_id={"grp": y_peer(k)}, device_id_type=MESH)

    @pl.when(f < n - 1)
    def _():
        pl.semaphore_signal(barrier, inc=1, device_id={"fs": f + 1}, device_id_type=MESH)

    @pl.when(f > 0)
    def _():
        pl.semaphore_signal(barrier, inc=1, device_id={"fs": f - 1}, device_id_type=MESH)

    neighbours = lax.min(f, 1) + lax.min(n - 1 - f, 1)
    pl.semaphore_wait(barrier, n_tp - 1 + parts - 1 + neighbours)

    def z_slot(blk, step):
        return lax.select((blk == f) & (step < 0), n, blk)

    def half_block(w, blk):
        size = own[w].shape[0] // parts
        at_rows = pl.ds(pl.multiple_of(g * size, 8), size)
        if w == GATE:
            return pair_full.at[:, blk, at_rows, :]
        return full[w].at[blk, at_rows, :]

    def z_sent(w, blk, step):
        half = half_block(w, blk)
        pltpu.make_async_remote_copy(
            src_ref=half, dst_ref=half, send_sem=z_send.at[ranks[w], z_slot(blk, step)], recv_sem=z_recv.at[bases[w], 0],
            device_id={"fs": f + step}, device_id_type=MESH,
        ).wait_send()

    def y_sent(w, blk, k):
        half = half_block(w, blk)
        pltpu.make_async_remote_copy(
            src_ref=half, dst_ref=half, send_sem=y_send.at[ranks[w], blk, k - 1], recv_sem=y_recv.at[bases[w], 0, k - 1],
            device_id={"grp": y_peer(k)}, device_id_type=MESH,
        ).wait_send()

    def seat(blk, host):
        return blk - lax.select(blk > host, 1, 0)

    def z_copy(w, c, blk, src, dst, step, host):
        return pltpu.make_async_remote_copy(
            src_ref=src, dst_ref=dst, send_sem=z_send.at[ranks[w], z_slot(blk, step)],
            recv_sem=z_recv.at[bases[w] + c, seat(blk, host)],
            device_id={"fs": f + step}, device_id_type=MESH,
        )

    def y_copy(w, c, blk, half, k, peer):
        return pltpu.make_async_remote_copy(
            src_ref=region(w, blk, half, c), dst_ref=region(w, blk, half, c),
            send_sem=y_send.at[ranks[w], blk, k - 1], recv_sem=y_recv.at[bases[w] + c, seat(blk, f), k - 1],
            device_id={"grp": peer}, device_id_type=MESH,
        )

    first_host, last_host = 1, n - 2
    is_host = (f >= first_host) & (f <= last_host)
    inner = lax.select(2 * f + 1 < n, 1, -1)

    def start_own(w, c):
        def towards(step):
            for v in members(w):
                z_copy(w, c, f, piece_of(v, g, c), landing(v, f, g, c), step, f + step).start()

        pl.when(f + 1 <= last_host)(lambda: towards(1))
        pl.when(f - 1 >= first_host)(lambda: towards(-1))

    def start_other(w, c):
        inward = lax.select(f == 0, 1, n - 2)
        for k in range(1, parts):
            half = lax.rem(g + parts - k, parts)
            for v in members(w):
                pltpu.make_async_remote_copy(
                    src_ref=piece_of(v, half, c), dst_ref=landing(v, f, half, c),
                    send_sem=y_send.at[ranks[w], f, k - 1],
                    recv_sem=y_recv.at[bases[w] + c, seat(f, inward), k - 1],
                    device_id={"fs": inward}, device_id_type=MESH,
                ).start()

    def direct(w):
        return w >= SHARED

    def relay(w, c, s, toward, next_to_edge):
        blk = f + toward * (1 + s)
        step = -toward

        @pl.when((blk >= 0) & (blk < n))
        def _():
            here = region(w, blk, g, c)
            z_copy(w, c, blk, here, here, step, f).wait_recv()

            def share():
                for k in range(1, parts):
                    y_copy(w, c, blk, g, k, y_peer(k)).start()

            def onward():
                z_copy(w, c, blk, here, here, step, f + step).start()

            pl.when((f + step <= last_host) & (f + step >= first_host))(onward)
            if next_to_edge and direct(w):
                pl.when((blk > 0) & (blk < n - 1))(share)
            else:
                share()

    def from_inner(w, c):
        relay(w, c, 0, inner, True)

    def from_outer(w, c):
        relay(w, c, 0, -inner, True)

    def from_far(w, c):
        @pl.loop(1, n - 2)
        def _(s):
            relay(w, c, s, inner, False)
            relay(w, c, s, -inner, False)

    def finish(w, c, blk):
        for k in range(1, parts):
            source = lax.rem(g + parts - k, parts)
            y_copy(w, c, blk, source, k, source).wait_recv()

    def finish_all(w, c):
        @pl.loop(0, n)
        def _(blk):
            pl.when(blk != f)(lambda: finish(w, c, blk))

    def own_copy(w):
        return pltpu.make_async_copy(own[w], full[w].at[f], own_sem.at[w])

    def own_columns(owner):
        return pl.ds(pl.multiple_of(owner * columns, 128), columns)

    chips = n_tp // 2
    core = lax.rem(t, 2)
    pair = t + 1 - 2 * core

    def ahead(k, start=None):
        return lax.rem((t if start is None else start) + 2 * k, n_tp)

    def behind(k, start=None):
        return lax.rem((t if start is None else start) + n_tp - 2 * k, n_tp)

    def set_rows(r):
        return pl.ds(r * rows, rows)

    def pair_copy(stage, r, k, src, dst):
        return pltpu.make_async_remote_copy(
            src_ref=src, dst_ref=dst, send_sem=pair_ss.at[stage, r, k], recv_sem=pair_rs.at[stage, r, k],
            device_id={"tp": pair}, device_id_type=MESH,
        )

    def far_copy(stage, r, k, src, dst, peer):
        return pltpu.make_async_remote_copy(
            src_ref=src, dst_ref=dst, send_sem=far_ss.at[stage, r, k], recv_sem=far_rs.at[stage, r, k],
            device_id={"tp": peer}, device_id_type=MESH,
        )

    def block_of(buf, r, owner):
        return buf.at[set_rows(r), own_columns(owner)]

    def gather_send(buf, stage, r):
        mine = block_of(buf, r, t)
        for k in range(1, chips):
            far_copy(stage, r, k, mine, mine, ahead(k)).start()
        pair_copy(stage, r, 0, mine, mine).start()

    def gather_relay(buf, stage, r):
        for k in range(1, chips):
            theirs = block_of(buf, r, behind(k))
            far_copy(stage, r, k, theirs, theirs, behind(k)).wait_recv()
            pair_copy(stage, r, k, theirs, theirs).start()

    def gather_finish(buf, stage, r):
        for k in range(chips):
            theirs = block_of(buf, r, behind(k, pair))
            pair_copy(stage, r, k, theirs, theirs).wait_recv()

    def gather_sent(buf, stage, r):
        mine = block_of(buf, r, t)
        for k in range(1, chips):
            far_copy(stage, r, k, mine, mine, ahead(k)).wait_send()
        for k in range(chips):
            pair_copy(stage, r, k, mine, mine).wait_send()

    def to_pair(r, k):
        return pair_copy(1, r, k, block_of(part, r, ahead(k, pair)), pair_recv.at[r, k])

    def to_far(r, k):
        return far_copy(1, r, k, block_of(part, r, ahead(k)), far_recv.at[r, k], ahead(k))

    def sum_send(r):
        for k in range(chips - 1, -1, -1):
            to_pair(r, k).start()

    def sum_relay(r):
        for k in range(1, chips):
            to_pair(r, k).wait_recv()

            @pl.loop(0, rows // 64)
            def _(i):
                inside = pl.ds(pl.multiple_of(i * 64, 64), 64)
                at = pl.ds(pl.multiple_of(r * rows + i * 64, 64), 64)
                both = part[at, own_columns(ahead(k))].astype(F32) + pair_recv[r, k, inside, :].astype(F32)
                part[at, own_columns(ahead(k))] = both.astype(BF16)

            to_far(r, k).start()

    def summed(r, start, size):
        inside = pl.ds(pl.multiple_of(start, size), size)
        at = pl.ds(pl.multiple_of(r * rows + start, size), size)
        total = part[at, own_columns(t)].astype(F32) + pair_recv[r, 0, inside, :].astype(F32)
        for k in range(1, chips):
            total = total + far_recv[r, k, inside, :].astype(F32)
        return at, total

    def first_rows(r):
        to_pair(r, 0).wait_recv()
        for k in range(1, chips):
            to_far(r, k).wait_recv()

        @pl.loop(0, rows // 64)
        def _(i):
            at, total = summed(r, i * 64, 64)
            first_full[at, own_columns(t)] = (tok_full[at, own_columns(t)].astype(F32) + total).astype(BF16)

    def norm_rows(source, gain, r):
        size = 32

        @pl.loop(0, rows // size)
        def _(i):
            at = pl.ds(pl.multiple_of(r * rows + i * size, size), size)
            values = source[at, :].astype(F32)
            scale = lax.rsqrt(jnp.sum(values * values, axis=1, keepdims=True) / width + 1e-06)
            normed[at, :] = (values * scale * gain[...]).astype(BF16)

    channels = w0.shape[1]
    block = w3.shape[1]
    units = w4.shape[1]
    tap_count = taps_ref.shape[0]

    def project(w, r):
        weight = full[w][...].reshape(width, channels)
        proj[w] = jnp.dot(normed[set_rows(r), :], weight, preferred_element_type=F32).astype(BF16)

    def convolve():
        taps = taps_ref[:, pl.ds(pl.multiple_of(t * channels, 128), channels)]

        @pl.loop(0, seqs)
        def _(i):
            at = pl.ds(pl.multiple_of(i * length, length), length)
            product = proj[1, at, :].astype(F32) * proj[2, at, :].astype(F32)
            position = lax.broadcasted_iota(jnp.int32, product.shape, 0)
            conv = jnp.zeros_like(product)
            for offset in range(tap_count):
                shift = tap_count - 1 - offset
                moved = product if shift == 0 else jnp.where(position >= shift, pltpu.roll(product, shift, 0), 0.0)
                conv = conv + taps[offset : offset + 1, :] * moved
            gated[at, :] = (proj[0, at, :].astype(F32) * conv).astype(BF16)

    def mix(r):
        @pl.loop(0, n)
        def _(b):
            at = pl.ds(pl.multiple_of(b * block, 128), block)
            part[set_rows(r), at] = jnp.dot(gated[...], full[3][b], preferred_element_type=F32).astype(BF16)

    def hidden_tile(r, start, size):
        at = pl.ds(start, size)
        left = normed[set_rows(r), :]
        gate = jnp.dot(left, full[GATE][:, :, at].reshape(width, size), preferred_element_type=F32)
        upward = jnp.dot(left, full[UP][:, :, at].reshape(width, size), preferred_element_type=F32)
        hidden[set_rows(r), at] = (gate / (1.0 + jnp.exp(-gate)) * upward).astype(BF16)

    def hidden_tiles(c, r):
        first, total = spans[GATE][c]
        for offset in range(0, total, 256):
            hidden_tile(r, first + offset, min(256, total - offset))

    wide = w6.shape[1]
    piece = spans[DOWN][0][1]
    pieces = counts[DOWN]

    def down_to_pair(r, k, slot, start):
        inside = pl.ds(pl.multiple_of(slot * piece, 128), piece)
        return pltpu.make_async_remote_copy(
            src_ref=part.at[set_rows(r), pl.ds(start, piece)], dst_ref=pair_recv.at[r, k, :, inside],
            send_sem=down_pair_ss.at[r, k], recv_sem=down_pair_rs.at[r, k, slot],
            device_id={"tp": pair}, device_id_type=MESH,
        )

    def down_to_far(r, k, slot, start):
        inside = pl.ds(pl.multiple_of(slot * piece, 128), piece)
        return pltpu.make_async_remote_copy(
            src_ref=part.at[set_rows(r), pl.ds(start, piece)], dst_ref=far_recv.at[r, k, :, inside],
            send_sem=down_far_ss.at[r, k], recv_sem=down_far_rs.at[r, k, slot],
            device_id={"tp": lax.rem(t + 2 * k, n_tp)}, device_id_type=MESH,
        )

    def down_sent(r, k):
        whole = pair_recv.at[r, k]
        pltpu.make_async_remote_copy(
            src_ref=whole, dst_ref=whole, send_sem=down_pair_ss.at[r, k], recv_sem=down_pair_rs.at[r, k, 0],
            device_id={"tp": pair}, device_id_type=MESH,
        ).wait_send()
        if k > 0:
            pltpu.make_async_remote_copy(
                src_ref=whole, dst_ref=whole, send_sem=down_far_ss.at[r, k], recv_sem=down_far_rs.at[r, k, 0],
                device_id={"tp": lax.rem(t + 2 * k, n_tp)}, device_id_type=MESH,
            ).wait_send()

    def place(b, c):
        start = pl.multiple_of(b * wide + c * piece, 128)
        owner = (b * wide + c * piece) // columns
        slot = lax.rem(b * wide + c * piece, columns) // piece
        k = lax.rem(owner // 2 - t // 2 + chips, chips)
        return start, owner, slot, k, lax.rem(owner, 2) == core

    def down_product(b, r, offset, size):
        weight = full[DOWN][b, :, pl.ds(offset, size)]
        part[set_rows(r), pl.ds(pl.multiple_of(b * wide + offset, 128), size)] = jnp.dot(
            hidden[set_rows(r), :], weight, preferred_element_type=F32
        ).astype(BF16)

    def to_lane(b, c):
        start, owner, slot, k, lane = place(b, c)

        @pl.when(jnp.logical_not(lane))
        def _():
            for r in (1, 0):
                down_to_pair(r, k, slot, start).start()

    def combine(b, c):
        start, owner, slot, k, lane = place(b, c)

        @pl.when(lane & (k > 0))
        def _():
            inside = pl.ds(pl.multiple_of(slot * piece, 128), piece)
            for r in (1, 0):
                down_to_pair(r, k, slot, start).wait_recv()

                @pl.loop(0, rows // 64)
                def _(i):
                    here = pl.ds(pl.multiple_of(i * 64, 64), 64)
                    at = pl.ds(pl.multiple_of(r * rows + i * 64, 64), 64)
                    both = part[at, pl.ds(start, piece)].astype(F32) + pair_recv[r, k, here, inside].astype(F32)
                    part[at, pl.ds(start, piece)] = both.astype(BF16)

                down_to_far(r, k, slot, start).start()

    def back_copy(slot, device):
        at = pl.ds(pl.multiple_of(slot * piece, 128), piece)
        return pltpu.make_async_remote_copy(
            src_ref=returned.at[:, at], dst_ref=returned.at[:, at], send_sem=back_ss.at[0], recv_sem=back_rs.at[slot],
            device_id={"fs": device}, device_id_type=MESH,
        )

    def back_sent():
        pltpu.make_async_remote_copy(
            src_ref=returned, dst_ref=returned, send_sem=back_ss.at[0], recv_sem=back_rs.at[0],
            device_id={"fs": guest}, device_id_type=MESH,
        ).wait_send()

    def settle(b, c):
        start, owner, slot, k, lane = place(b, c)

        @pl.when(owner == t)
        def _():
            inside = pl.ds(pl.multiple_of(slot * piece, 128), piece)
            for r in (1, 0):
                down_to_pair(r, 0, slot, start).wait_recv()
                for far in range(1, chips):
                    down_to_far(r, far, slot, start).wait_recv()

                @pl.loop(0, rows // 64)
                def _(i):
                    here = pl.ds(pl.multiple_of(i * 64, 64), 64)
                    at = pl.ds(pl.multiple_of(r * rows + i * 64, 64), 64)
                    total = part[at, pl.ds(start, piece)].astype(F32) + pair_recv[r, 0, here, inside].astype(F32)
                    for far in range(1, chips):
                        total = total + far_recv[r, far, here, inside].astype(F32)
                    second = first_full[at, pl.ds(start, piece)].astype(F32) + total
                    squares = second * second
                    folded = squares[:, :128]
                    for lane_block in range(1, piece // 128):
                        folded = folded + squares[:, lane_block * 128 : (lane_block + 1) * 128]
                    sq_acc[at, :] += folded
                    if r == 0:
                        second_own[here, inside] = second
                    else:
                        returned[here, inside] = second.astype(BF16)

                if r == 1:
                    pl.when(has_guest)(lambda: back_copy(slot, guest).start())

    guest = lax.select(f == 1, 0, n - 1)

    def ahead_of(k):
        return lax.rem(t + k, n_tp)

    def square_copy(k, peer):
        return pltpu.make_async_remote_copy(
            src_ref=sq_send.at[0], dst_ref=sq_recv.at[0, k], send_sem=sq_ss.at[0, k],
            recv_sem=sq_rs.at[0, k], device_id={"tp": peer}, device_id_type=MESH,
        )

    def edge_squares(k, peer):
        return pltpu.make_async_remote_copy(
            src_ref=sq_send.at[1], dst_ref=sq_recv.at[1, k], send_sem=sq_ss.at[1, k],
            recv_sem=sq_rs.at[1, k], device_id={"fs": guest, "tp": peer}, device_id_type=MESH,
        )

    def squares_of(r):
        for i in range(seqs):
            at = pl.ds(r * rows + i * length, length)
            sums = jnp.sum(jnp.transpose(sq_acc[at, :]), axis=0, keepdims=True)
            sq_send[r, i] = jnp.broadcast_to(sums, (8, length))

    def squares_total():
        total = sq_send[0]
        for k in range(1, n_tp):
            square_copy(k, t).wait_recv()
            total = total + sq_recv[0, k]
        return total

    def close(values, squares):
        gain = out_gain[:, own_columns(t)]
        for i in range(seqs):
            factor = spread(lax.rsqrt(squares[i][:1, :] / width + 1e-06))
            inside = pl.ds(i * length, length)
            for start in range(0, columns, length):
                at = pl.ds(start, min(length, columns - start))
                scaled = values[inside, at].astype(F32) * factor[:, : at.size] * gain[:, start : start + at.size]
                out_ref[inside, at] = scaled.astype(BF16)

    has_guest = (f == 1) | (f == n - 2)
    inward = lax.select(f == 0, 1, n - 2)

    def tokens_in(device):
        return pltpu.make_async_remote_copy(
            src_ref=tok_ref, dst_ref=block_of(tok_full, 1, t), send_sem=guest_sem.at[0], recv_sem=guest_sem.at[1],
            device_id={"fs": device}, device_id_type=MESH,
        )

    @pl.when(jnp.logical_not(is_host))
    def _():
        small_copy(3).wait()
        order = [("own", w, 0) for w in range(MIXER)] + [("tokens", 0, 0)]
        order += [("other", w, 0) for w in range(MIXER) if direct(w)]
        for c in range(counts[GATE] + TRAIL):
            order += [("own", GATE, c)] if c < counts[GATE] else []
            order += [("other", GATE, c - TRAIL)] if c >= TRAIL else []
        for kind in ("own", "other"):
            order += [(kind, DOWN, c) for c in range(pieces)]
        for kind, w, c in order:
            if kind == "own":
                start_own(w, c)
            elif kind == "tokens":
                tokens_in(inward).start()
            else:
                start_other(w, c)
        tokens_in(inward).wait_send()
        for w in groups:
            z_sent(w, f, lax.select(f == 0, 1, -1))
            if direct(w):
                for k in range(1, parts):
                    y_sent(w, f, k)
        def take_back(slot):
            back_copy(slot, inward).wait_recv()

        def take_squares(k):
            edge_squares(k, t).wait_recv()

        for slot in range(columns // piece):
            take_back(slot)
        for k in range(n_tp):
            take_squares(k)
        sq_total[...] = sum(sq_recv[1, k] for k in range(1, n_tp)) + sq_recv[1, 0]
        close(returned, sq_total)

    @pl.when(is_host)
    def _():
        for w in range(MIXER):
            start_own(w, 0)
        for w in range(7):
            own_copy(w).start()
        own_tokens().wait()
        gather_send(tok_full, 0, 0)
        for i in range(4):
            small_copy(i).wait()
        sq_acc[...] = jnp.zeros_like(sq_acc)
        for w in range(MIXER):
            from_inner(w, 0)
            from_outer(w, 0)
        last = counts[GATE] - 1

        def start_pair(c):
            if c <= last:
                start_own(GATE, c)

        def inner_pair(c):
            if c <= last:
                from_inner(GATE, c)

        def outer_pair(c):
            if c <= last:
                from_outer(GATE, c)

        def far_pair(c):
            if c <= last:
                from_far(GATE, c)

        def start_down(first, end):
            for c in range(first, min(end, pieces)):
                start_own(DOWN, c)

        def inner_down(c):
            if c < pieces:
                from_inner(DOWN, c)

        def outer_down(c):
            if c < pieces:
                from_outer(DOWN, c)

        def tile(c, r):
            if c <= last:
                if r == 0:
                    finish_all(GATE, c)
                hidden_tiles(c, r)

        def drain(group):
            for w in group:
                @pl.loop(0, n)
                def _(blk):
                    pl.when((f + 1 <= last_host) & (blk <= f))(lambda: z_sent(w, blk, 1))
                    pl.when((f - 1 >= first_host) & (blk >= f))(lambda: z_sent(w, blk, -1))
                    whole = ((blk == 0) & (f == 1)) | ((blk == n - 1) & (f == n - 2))
                    relayed = (blk != f) & jnp.logical_not(whole) if direct(w) else blk != f

                    @pl.when(relayed)
                    def _():
                        for k in range(1, parts):
                            y_sent(w, blk, k)

        start_pair(0)
        start_pair(1)
        start_pair(2)
        gather_relay(tok_full, 0, 0)
        from_far(0, 0)
        gather_finish(tok_full, 0, 0)
        norm_rows(tok_full, mix_gain, 0)
        for w in range(1, MIXER):
            from_far(w, 0)

        @pl.when(has_guest)
        def _():
            tokens_in(guest).wait_recv()

        gather_send(tok_full, 0, 1)
        inner_pair(0)
        for w in range(3):
            own_copy(w).wait()
            finish_all(w, 0)
            project(w, 0)
        convolve()
        own_copy(3).wait()
        finish_all(3, 0)
        mix(0)
        sum_send(0)
        inner_pair(1)
        gather_relay(tok_full, 0, 1)
        gather_finish(tok_full, 0, 1)
        outer_pair(0)
        sum_relay(0)
        norm_rows(tok_full, mix_gain, 1)
        inner_pair(2)
        project(0, 1)
        project(1, 1)
        outer_pair(1)
        start_pair(3)
        project(2, 1)
        convolve()
        mix(1)
        sum_send(1)
        far_pair(0)
        sum_relay(1)
        outer_pair(2)
        start_pair(4)
        far_pair(1)
        first_rows(0)
        gather_send(first_full, 2, 0)
        inner_pair(3)
        outer_pair(3)
        start_pair(5)
        far_pair(2)
        first_rows(1)
        gather_send(first_full, 2, 1)
        inner_pair(4)
        outer_pair(4)
        start_down(0, 1)
        far_pair(3)
        for w in (GATE, UP):
            own_copy(w).wait()
        gather_relay(first_full, 2, 0)
        inner_pair(5)
        gather_finish(first_full, 2, 0)
        outer_pair(5)
        start_down(1, pieces)
        norm_rows(first_full, ffn_gain, 0)
        far_pair(4)
        tile(0, 0)
        tile(1, 0)
        far_pair(5)
        tile(2, 0)
        gather_relay(first_full, 2, 1)
        tile(3, 0)
        inner_down(0)
        gather_finish(first_full, 2, 1)
        norm_rows(first_full, ffn_gain, 1)
        for r in range(2):
            for k in range(chips):
                to_pair(r, k).wait_send()
            for k in range(1, chips):
                to_far(r, k).wait_send()
        tile(0, 1)
        tile(1, 1)
        inner_down(1)
        tile(2, 1)
        tile(3, 1)
        inner_down(2)
        tile(4, 0)
        outer_down(0)
        tile(4, 1)
        tile(5, 0)
        inner_down(3)
        outer_down(1)
        tile(5, 1)
        for c in range(6, last + 1):
            start_pair(c)
            inner_pair(c)
            outer_pair(c)
            far_pair(c)
            tile(c, 0)
            tile(c, 1)
        own_copy(DOWN).wait()
        near, outer = f + inner, f - inner
        batch = 2 if pieces % 2 == 0 else 1

        def produce(b, first, count):
            for r in (1, 0):
                down_product(b, r, pl.multiple_of(first * piece, 128), count * piece)
            for i in range(count):
                to_lane(b, first + i)

        def far_down(c):
            if c < pieces:
                from_far(DOWN, c)

        def join(b, first, count):
            for c in range(first, first + count):
                combine(b, c)

        def near_pieces(first, count):
            for c in range(first, first + count):
                finish(DOWN, c, near)
            produce(near, first, count)

        produce(f, 0, batch)
        near_pieces(0, batch)
        outer_down(2)
        join(f, 0, batch)
        join(near, 0, batch)
        far_down(0)
        for first in range(batch, pieces, batch):
            produce(f, first, batch)
            near_pieces(first, batch)
            join(f, first, batch)
            join(near, first, batch)
        far_down(1)
        for c in range(3, pieces):
            outer_down(c)
        far_down(2)
        drain(groups[:-1])
        for r in range(2):
            gather_sent(tok_full, 0, r)
            gather_sent(first_full, 2, r)

        def others(visit):
            @pl.loop(1, n - 2)
            def _(s):
                for toward in (inner, -inner):
                    b = f + toward * (1 + s)
                    pl.when((b >= 0) & (b < n))(lambda: visit(b))

        def take(b, first, count):
            for c in range(first, first + count):
                finish(DOWN, c, b)
            produce(b, first, count)

        def settle_range(first, end):
            @pl.loop(first, end)
            def _(i):
                settle(f, i)
                settle(near, i)

        def far_take(c):
            others(lambda b: take(b, c, 1))

        def far_join(c):
            others(lambda b: combine(b, c))

        far_take(0)
        far_join(0)
        take(outer, 0, batch)
        for c in range(3, pieces):
            from_far(DOWN, c)
        for c in range(1, batch):
            far_take(c)
        join(outer, 0, batch)
        settle_range(0, batch)
        for c in range(1, batch):
            far_join(c)
        for c in range(batch, pieces):
            take(outer, c, 1)
            if c > batch:
                far_join(c - 1)
            join(outer, c, 1)
            if c == batch:
                settle_range(batch, pieces)
            far_take(c)
        if pieces > batch:
            far_join(pieces - 1)
            for c in range(batch):
                settle(outer, c)
        for c in range(pieces):
            others(lambda b: settle(b, c))
            if c >= batch or pieces == batch:
                settle(outer, c)

        squares_of(1)

        @pl.when(has_guest)
        def _():
            for k in range(n_tp):
                edge_squares(k, ahead_of(k)).start()

        squares_of(0)
        for k in range(1, n_tp):
            square_copy(k, ahead_of(k)).start()
        sq_total[...] = squares_total()
        close(second_own, sq_total)

        @pl.when(has_guest)
        def _():
            for k in range(n_tp):
                edge_squares(k, ahead_of(k)).wait_send()
            back_sent()

        for k in range(1, n_tp):
            square_copy(k, ahead_of(k)).wait_send()
        for r in range(2):
            for k in range(chips):
                down_sent(r, k)
        drain((DOWN,))


def solution(mesh):
    n, parts, n_tp = mesh.shape["fs"], mesh.shape["grp"], mesh.shape["tp"]

    def local(tokens, mix_gain, outer, inner, value, taps, mix_out, ffn_gain, gate, up, down, out_gain):
        seqs, length, columns = tokens.shape
        rows, width = seqs * length, columns * n_tp
        weights = (outer, inner, value, mix_out, gate, up, down)
        piece = min(down.shape[1], columns, 128)
        spans = [((0, a.shape[1]),) for a in weights]
        spans[GATE] = spans[UP] = tiles_of(gate.shape[1])
        spans[DOWN] = tuple((start, piece) for start in range(0, down.shape[1], piece))
        slots = sum(len(tiles) for w, tiles in enumerate(spans) if w != UP)
        groups = len(weights) - 1
        channels, units = outer.shape[1], gate.shape[1]
        y_others = max(parts - 1, 1)
        per_owner = columns // piece
        dma = pltpu.SemaphoreType.DMA
        scratch = [pltpu.VMEM((n,) + a.shape, BF16) for a in weights[:GATE]]
        scratch += [pltpu.VMEM((2, n) + gate.shape, BF16), pltpu.VMEM((n,) + down.shape, BF16)]
        chips = n_tp // 2
        scratch += [
            pltpu.VMEM((2 * rows, width), BF16),
            pltpu.VMEM((2 * rows, width), BF16),
            pltpu.VMEM((3, rows, channels), BF16),
            pltpu.VMEM((rows, channels), BF16),
            pltpu.VMEM((2 * rows, width), BF16),
            pltpu.VMEM((2, chips, rows, columns), BF16),
            pltpu.VMEM((2, chips, rows, columns), BF16),
            pltpu.VMEM((2 * rows, width), BF16),
            pltpu.VMEM((2 * rows, units), BF16),
            pltpu.VMEM((rows, columns), BF16),
            pltpu.VMEM((rows, columns), F32),
            pltpu.VMEM((2 * rows, 128), F32),
            pltpu.VMEM((2, seqs, 8, length), F32),
            pltpu.VMEM((2, n_tp, seqs, 8, length), F32),
            pltpu.VMEM((seqs, 8, length), F32),
            pltpu.VMEM((1, width), F32), pltpu.VMEM(taps.shape, F32),
            pltpu.VMEM((1, width), F32), pltpu.VMEM((1, width), F32),
            dma((groups, n + 1)), dma((slots, n - 1)),
            dma((groups, n, y_others)), dma((slots, n - 1, y_others)),
            dma((12,)), dma((3, 2, chips)), dma((3, 2, chips)), dma((3, 2, chips)), dma((3, 2, chips)),
            dma((2, chips)), dma((2, chips, per_owner)), dma((2, chips)), dma((2, chips, per_owner)),
            dma((2, n_tp)), dma((2, n_tp)), dma((1,)), dma((per_owner,)), dma((2,)),
        ]
        out = pl.pallas_call(
            functools.partial(kernel, n, parts, n_tp, length, tuple(spans)),
            out_shape=jax.ShapeDtypeStruct((rows, columns), BF16),
            in_specs=[pl.BlockSpec(memory_space=pl.ANY)] * 12,
            out_specs=pl.BlockSpec(memory_space=pltpu.VMEM),
            scratch_shapes=scratch,
            compiler_params=pltpu.CompilerParams(
                collective_id=0, has_side_effects=True, vmem_limit_bytes=62 * 1024 * 1024
            ),
        )(
            tokens.reshape(rows, columns), mix_gain[None], outer, inner, value, taps, mix_out,
            ffn_gain[None], gate, up, down, out_gain[None],
        )
        return out.reshape(seqs, length, columns)

    in_specs = (
        P(("grp", "fs"), None, "tp"), P(), P("fs", "tp"), P("fs", "tp"), P("fs", "tp"), P(), P("tp", "fs"),
        P(), P("fs", "tp"), P("fs", "tp"), P("tp", "fs"), P(),
    )
    out_specs = P(("grp", "fs"), None, "tp")
    return jax.shard_map(local, mesh=mesh, in_specs=in_specs, out_specs=out_specs, check_vma=False)
```

```python
import functools

import jax
import jax.numpy as jnp
from jax import lax
from jax.experimental import pallas as pl
from jax.experimental.pallas import tpu as pltpu
from jax.sharding import PartitionSpec as P

MESH = pl.DeviceIdType.MESH
F32 = jnp.float32
BF16 = jnp.bfloat16
MIXER = 4
GATE, UP, DOWN = 4, 5, 6
SHARED = 1
TRAIL = 2
LAG = 2


def tiles_of(units):
    if units % 128:
        return ((0, units),)
    return tuple((start, min(256, units - start)) for start in range(0, units, 256))


def spread(rows):
    return jnp.transpose(jnp.broadcast_to(rows, (rows.shape[1], rows.shape[1])))


def kernel(
    n, parts, n_tp, length, spans,
    tok_ref, mix_gain_in, w0, w1, w2, taps_in, w3, ffn_gain_in, w4, w5, w6, out_gain_in,
    out_hbm,
    f0, f1, f2, f3, pair_full, f6,
    tok_full, normed, proj, gated, part, pair_recv, far_recv, first_full, hidden, returned, second_own, sq_acc,
    sq_send, sq_recv, sq_total, out_ref, mix_gain, taps_ref, ffn_gain, out_gain,
    z_send, z_recv, y_send, y_recv, own_sem, pair_ss, pair_rs, far_ss, far_rs,
    down_pair_ss, down_pair_rs, down_far_ss, down_far_rs, sq_ss, sq_rs, back_ss, back_rs, guest_sem, out_sem,
):
    own = (w0, w1, w2, w3, w4, w5, w6)
    full = (f0, f1, f2, f3, pair_full.at[0], pair_full.at[1], f6)
    f, g, t = lax.axis_index("fs"), lax.axis_index("grp"), lax.axis_index("tp")
    rows, columns = tok_ref.shape
    width = columns * n_tp
    seqs = rows // length
    counts = [len(tiles) for tiles in spans]
    groups = (0, 1, 2, 3, GATE, DOWN)
    ranks = {w: i for i, w in enumerate(groups)}
    bases = {w: sum(counts[v] for v in groups[:i]) for w, i in ranks.items()}

    def y_peer(k):
        return lax.rem(g + k, parts)

    def tp_peer(k):
        return lax.rem(t + k, n_tp)

    def span(w, half, c):
        size = own[w].shape[0] // parts
        if isinstance(c, int):
            at = pl.ds(*spans[w][c])
        else:
            width_c = spans[w][0][1]
            at = pl.ds(pl.multiple_of(c * width_c, 128), width_c)
        return pl.ds(pl.multiple_of(half * size, 8), size), at

    def members(w):
        return (GATE, UP) if w == GATE else (w,)

    def region(w, blk, half, c):
        at_rows, at_cols = span(w, half, c)
        if w == GATE:
            return pair_full.at[:, blk, at_rows, at_cols]
        return full[w].at[blk, at_rows, at_cols]

    def landing(v, blk, half, c):
        at_rows, at_cols = span(v, half, c)
        if v in (GATE, UP):
            return pair_full.at[v - GATE, blk, at_rows, at_cols]
        return full[v].at[blk, at_rows, at_cols]

    def piece_of(w, half, c):
        at_rows, at_cols = span(w, half, c)
        return own[w].at[at_rows, at_cols]

    def small_copy(i):
        pairs = ((mix_gain_in, mix_gain), (taps_in, taps_ref), (ffn_gain_in, ffn_gain), (out_gain_in, out_gain))
        return pltpu.make_async_copy(*pairs[i], own_sem.at[8 + i])

    def own_tokens():
        mine = tok_full.at[pl.ds(0, rows), pl.ds(pl.multiple_of(t * columns, 128), columns)]
        return pltpu.make_async_copy(tok_ref, mine, own_sem.at[7])

    hosting = (f >= 1) & (f <= n - 2)
    small_copy(3).start()

    @pl.when(hosting)
    def _():
        own_tokens().start()
        for i in range(3):
            small_copy(i).start()

    barrier = pltpu.get_barrier_semaphore()
    for k in range(1, n_tp):
        pl.semaphore_signal(barrier, inc=1, device_id={"tp": tp_peer(k)}, device_id_type=MESH)
    for k in range(1, parts):
        pl.semaphore_signal(barrier, inc=1, device_id={"grp": y_peer(k)}, device_id_type=MESH)

    @pl.when(f < n - 1)
    def _():
        pl.semaphore_signal(barrier, inc=1, device_id={"fs": f + 1}, device_id_type=MESH)

    @pl.when(f > 0)
    def _():
        pl.semaphore_signal(barrier, inc=1, device_id={"fs": f - 1}, device_id_type=MESH)

    neighbours = lax.min(f, 1) + lax.min(n - 1 - f, 1)
    pl.semaphore_wait(barrier, n_tp - 1 + parts - 1 + neighbours)

    def z_slot(blk, step):
        return lax.select((blk == f) & (step < 0), n, blk)

    def half_block(w, blk):
        size = own[w].shape[0] // parts
        at_rows = pl.ds(pl.multiple_of(g * size, 8), size)
        if w == GATE:
            return pair_full.at[:, blk, at_rows, :]
        return full[w].at[blk, at_rows, :]

    def z_sent(w, blk, step):
        half = half_block(w, blk)
        pltpu.make_async_remote_copy(
            src_ref=half, dst_ref=half, send_sem=z_send.at[ranks[w], z_slot(blk, step)], recv_sem=z_recv.at[bases[w], 0],
            device_id={"fs": f + step}, device_id_type=MESH,
        ).wait_send()

    def y_sent(w, blk, k):
        half = half_block(w, blk)
        pltpu.make_async_remote_copy(
            src_ref=half, dst_ref=half, send_sem=y_send.at[ranks[w], blk, k - 1], recv_sem=y_recv.at[bases[w], 0, k - 1],
            device_id={"grp": y_peer(k)}, device_id_type=MESH,
        ).wait_send()

    def seat(blk, host):
        return blk - lax.select(blk > host, 1, 0)

    def z_copy(w, c, blk, src, dst, step, host):
        return pltpu.make_async_remote_copy(
            src_ref=src, dst_ref=dst, send_sem=z_send.at[ranks[w], z_slot(blk, step)],
            recv_sem=z_recv.at[bases[w] + c, seat(blk, host)],
            device_id={"fs": f + step}, device_id_type=MESH,
        )

    def y_copy(w, c, blk, half, k, peer):
        return pltpu.make_async_remote_copy(
            src_ref=region(w, blk, half, c), dst_ref=region(w, blk, half, c),
            send_sem=y_send.at[ranks[w], blk, k - 1], recv_sem=y_recv.at[bases[w] + c, seat(blk, f), k - 1],
            device_id={"grp": peer}, device_id_type=MESH,
        )

    first_host, last_host = 1, n - 2
    is_host = (f >= first_host) & (f <= last_host)
    inner = lax.select(2 * f + 1 < n, 1, -1)

    def start_own(w, c):
        def towards(step):
            for v in members(w):
                z_copy(w, c, f, piece_of(v, g, c), landing(v, f, g, c), step, f + step).start()

        pl.when(f + 1 <= last_host)(lambda: towards(1))
        pl.when(f - 1 >= first_host)(lambda: towards(-1))

    def start_other(w, c):
        inward = lax.select(f == 0, 1, n - 2)
        for k in range(1, parts):
            half = lax.rem(g + parts - k, parts)
            for v in members(w):
                pltpu.make_async_remote_copy(
                    src_ref=piece_of(v, half, c), dst_ref=landing(v, f, half, c),
                    send_sem=y_send.at[ranks[w], f, k - 1],
                    recv_sem=y_recv.at[bases[w] + c, seat(f, inward), k - 1],
                    device_id={"fs": inward}, device_id_type=MESH,
                ).start()

    def direct(w):
        return w >= SHARED

    def relay(w, c, s, toward, next_to_edge):
        blk = f + toward * (1 + s)
        step = -toward

        @pl.when((blk >= 0) & (blk < n))
        def _():
            here = region(w, blk, g, c)
            z_copy(w, c, blk, here, here, step, f).wait_recv()

            def share():
                for k in range(1, parts):
                    y_copy(w, c, blk, g, k, y_peer(k)).start()

            def onward():
                z_copy(w, c, blk, here, here, step, f + step).start()

            pl.when((f + step <= last_host) & (f + step >= first_host))(onward)
            if next_to_edge and direct(w):
                pl.when((blk > 0) & (blk < n - 1))(share)
            else:
                share()

    def from_inner(w, c):
        relay(w, c, 0, inner, True)

    def from_outer(w, c):
        relay(w, c, 0, -inner, True)

    def from_far(w, c):
        @pl.loop(1, n - 2)
        def _(s):
            relay(w, c, s, inner, False)
            relay(w, c, s, -inner, False)

    def finish(w, c, blk):
        for k in range(1, parts):
            source = lax.rem(g + parts - k, parts)
            y_copy(w, c, blk, source, k, source).wait_recv()

    def finish_all(w, c):
        @pl.loop(0, n)
        def _(blk):
            pl.when(blk != f)(lambda: finish(w, c, blk))

    def own_copy(w):
        return pltpu.make_async_copy(own[w], full[w].at[f], own_sem.at[w])

    def own_columns(owner):
        return pl.ds(pl.multiple_of(owner * columns, 128), columns)

    chips = n_tp // 2
    core = lax.rem(t, 2)
    pair = t + 1 - 2 * core

    def ahead(k, start=None):
        return lax.rem((t if start is None else start) + 2 * k, n_tp)

    def behind(k, start=None):
        return lax.rem((t if start is None else start) + n_tp - 2 * k, n_tp)

    def set_rows(r):
        return pl.ds(r * rows, rows)

    def pair_copy(stage, r, k, src, dst):
        return pltpu.make_async_remote_copy(
            src_ref=src, dst_ref=dst, send_sem=pair_ss.at[stage, r, k], recv_sem=pair_rs.at[stage, r, k],
            device_id={"tp": pair}, device_id_type=MESH,
        )

    def far_copy(stage, r, k, src, dst, peer):
        return pltpu.make_async_remote_copy(
            src_ref=src, dst_ref=dst, send_sem=far_ss.at[stage, r, k], recv_sem=far_rs.at[stage, r, k],
            device_id={"tp": peer}, device_id_type=MESH,
        )

    def block_of(buf, r, owner):
        return buf.at[set_rows(r), own_columns(owner)]

    def gather_send(buf, stage, r):
        mine = block_of(buf, r, t)
        for k in range(1, chips):
            far_copy(stage, r, k, mine, mine, ahead(k)).start()
        pair_copy(stage, r, 0, mine, mine).start()

    def gather_relay(buf, stage, r):
        for k in range(1, chips):
            theirs = block_of(buf, r, behind(k))
            far_copy(stage, r, k, theirs, theirs, behind(k)).wait_recv()
            pair_copy(stage, r, k, theirs, theirs).start()

    def gather_finish(buf, stage, r):
        for k in range(chips):
            theirs = block_of(buf, r, behind(k, pair))
            pair_copy(stage, r, k, theirs, theirs).wait_recv()

    def gather_sent(buf, stage, r):
        mine = block_of(buf, r, t)
        for k in range(1, chips):
            far_copy(stage, r, k, mine, mine, ahead(k)).wait_send()
        for k in range(chips):
            pair_copy(stage, r, k, mine, mine).wait_send()

    def to_pair(r, k):
        return pair_copy(1, r, k, block_of(part, r, ahead(k, pair)), pair_recv.at[r, k])

    def to_far(r, k):
        return far_copy(1, r, k, block_of(part, r, ahead(k)), far_recv.at[r, k], ahead(k))

    def sum_send(r):
        for k in range(chips - 1, -1, -1):
            to_pair(r, k).start()

    def sum_relay(r):
        for k in range(1, chips):
            to_pair(r, k).wait_recv()

            @pl.loop(0, rows // 64)
            def _(i):
                inside = pl.ds(pl.multiple_of(i * 64, 64), 64)
                at = pl.ds(pl.multiple_of(r * rows + i * 64, 64), 64)
                both = part[at, own_columns(ahead(k))].astype(F32) + pair_recv[r, k, inside, :].astype(F32)
                part[at, own_columns(ahead(k))] = both.astype(BF16)

            to_far(r, k).start()

    def summed(r, start, size):
        inside = pl.ds(pl.multiple_of(start, size), size)
        at = pl.ds(pl.multiple_of(r * rows + start, size), size)
        total = part[at, own_columns(t)].astype(F32) + pair_recv[r, 0, inside, :].astype(F32)
        for k in range(1, chips):
            total = total + far_recv[r, k, inside, :].astype(F32)
        return at, total

    def first_rows(r):
        to_pair(r, 0).wait_recv()
        for k in range(1, chips):
            to_far(r, k).wait_recv()

        @pl.loop(0, rows // 64)
        def _(i):
            at, total = summed(r, i * 64, 64)
            first_full[at, own_columns(t)] = (tok_full[at, own_columns(t)].astype(F32) + total).astype(BF16)

    def norm_rows(source, gain, r):
        size = 32

        @pl.loop(0, rows // size)
        def _(i):
            at = pl.ds(pl.multiple_of(r * rows + i * size, size), size)
            values = source[at, :].astype(F32)
            scale = lax.rsqrt(jnp.sum(values * values, axis=1, keepdims=True) / width + 1e-06)
            normed[at, :] = (values * scale * gain[...]).astype(BF16)

    channels = w0.shape[1]
    block = w3.shape[1]
    units = w4.shape[1]
    tap_count = taps_ref.shape[0]

    def project(w, r):
        weight = full[w][...].reshape(width, channels)
        proj[w] = jnp.dot(normed[set_rows(r), :], weight, preferred_element_type=F32).astype(BF16)

    def convolve():
        taps = taps_ref[:, pl.ds(pl.multiple_of(t * channels, 128), channels)]

        @pl.loop(0, seqs)
        def _(i):
            at = pl.ds(pl.multiple_of(i * length, length), length)
            product = proj[1, at, :].astype(F32) * proj[2, at, :].astype(F32)
            position = lax.broadcasted_iota(jnp.int32, product.shape, 0)
            conv = jnp.zeros_like(product)
            for offset in range(tap_count):
                shift = tap_count - 1 - offset
                moved = product if shift == 0 else jnp.where(position >= shift, pltpu.roll(product, shift, 0), 0.0)
                conv = conv + taps[offset : offset + 1, :] * moved
            gated[at, :] = (proj[0, at, :].astype(F32) * conv).astype(BF16)

    def mix(r):
        @pl.loop(0, n)
        def _(b):
            at = pl.ds(pl.multiple_of(b * block, 128), block)
            part[set_rows(r), at] = jnp.dot(gated[...], full[3][b], preferred_element_type=F32).astype(BF16)

    def hidden_tile(r, start, size):
        at = pl.ds(start, size)
        left = normed[set_rows(r), :]
        gate = jnp.dot(left, full[GATE][:, :, at].reshape(width, size), preferred_element_type=F32)
        upward = jnp.dot(left, full[UP][:, :, at].reshape(width, size), preferred_element_type=F32)
        hidden[set_rows(r), at] = (gate / (1.0 + jnp.exp(-gate)) * upward).astype(BF16)

    def hidden_tiles(c, r):
        first, total = spans[GATE][c]
        for offset in range(0, total, 256):
            hidden_tile(r, first + offset, min(256, total - offset))

    wide = w6.shape[1]
    piece = spans[DOWN][0][1]
    pieces = counts[DOWN]

    def down_to_pair(r, k, slot, start):
        inside = pl.ds(pl.multiple_of(slot * piece, 128), piece)
        return pltpu.make_async_remote_copy(
            src_ref=part.at[set_rows(r), pl.ds(start, piece)], dst_ref=pair_recv.at[r, k, :, inside],
            send_sem=down_pair_ss.at[r, k], recv_sem=down_pair_rs.at[r, k, slot],
            device_id={"tp": pair}, device_id_type=MESH,
        )

    def down_to_far(r, k, slot, start):
        inside = pl.ds(pl.multiple_of(slot * piece, 128), piece)
        return pltpu.make_async_remote_copy(
            src_ref=part.at[set_rows(r), pl.ds(start, piece)], dst_ref=far_recv.at[r, k, :, inside],
            send_sem=down_far_ss.at[r, k], recv_sem=down_far_rs.at[r, k, slot],
            device_id={"tp": lax.rem(t + 2 * k, n_tp)}, device_id_type=MESH,
        )

    def down_sent(r, k):
        whole = pair_recv.at[r, k]
        pltpu.make_async_remote_copy(
            src_ref=whole, dst_ref=whole, send_sem=down_pair_ss.at[r, k], recv_sem=down_pair_rs.at[r, k, 0],
            device_id={"tp": pair}, device_id_type=MESH,
        ).wait_send()
        if k > 0:
            pltpu.make_async_remote_copy(
                src_ref=whole, dst_ref=whole, send_sem=down_far_ss.at[r, k], recv_sem=down_far_rs.at[r, k, 0],
                device_id={"tp": lax.rem(t + 2 * k, n_tp)}, device_id_type=MESH,
            ).wait_send()

    def place(b, c):
        start = pl.multiple_of(b * wide + c * piece, 128)
        owner = (b * wide + c * piece) // columns
        slot = lax.rem(b * wide + c * piece, columns) // piece
        k = lax.rem(owner // 2 - t // 2 + chips, chips)
        return start, owner, slot, k, lax.rem(owner, 2) == core

    def down_product(b, r, offset, size):
        weight = full[DOWN][b, :, pl.ds(offset, size)]
        part[set_rows(r), pl.ds(pl.multiple_of(b * wide + offset, 128), size)] = jnp.dot(
            hidden[set_rows(r), :], weight, preferred_element_type=F32
        ).astype(BF16)

    def to_lane(b, c):
        start, owner, slot, k, lane = place(b, c)

        @pl.when(jnp.logical_not(lane))
        def _():
            for r in (1, 0):
                down_to_pair(r, k, slot, start).start()

    def combine(b, c):
        start, owner, slot, k, lane = place(b, c)

        @pl.when(lane & (k > 0))
        def _():
            inside = pl.ds(pl.multiple_of(slot * piece, 128), piece)
            for r in (1, 0):
                down_to_pair(r, k, slot, start).wait_recv()

                @pl.loop(0, rows // 64)
                def _(i):
                    here = pl.ds(pl.multiple_of(i * 64, 64), 64)
                    at = pl.ds(pl.multiple_of(r * rows + i * 64, 64), 64)
                    both = part[at, pl.ds(start, piece)].astype(F32) + pair_recv[r, k, here, inside].astype(F32)
                    part[at, pl.ds(start, piece)] = both.astype(BF16)

                down_to_far(r, k, slot, start).start()

    def back_copy(slot, device):
        at = pl.ds(pl.multiple_of(slot * piece, 128), piece)
        return pltpu.make_async_remote_copy(
            src_ref=returned.at[:, at], dst_ref=returned.at[:, at], send_sem=back_ss.at[0], recv_sem=back_rs.at[slot],
            device_id={"fs": device}, device_id_type=MESH,
        )

    def back_sent():
        pltpu.make_async_remote_copy(
            src_ref=returned, dst_ref=returned, send_sem=back_ss.at[0], recv_sem=back_rs.at[0],
            device_id={"fs": guest}, device_id_type=MESH,
        ).wait_send()

    def settle(b, c):
        start, owner, slot, k, lane = place(b, c)

        @pl.when(owner == t)
        def _():
            inside = pl.ds(pl.multiple_of(slot * piece, 128), piece)
            for r in (1, 0):
                down_to_pair(r, 0, slot, start).wait_recv()
                for far in range(1, chips):
                    down_to_far(r, far, slot, start).wait_recv()

                @pl.loop(0, rows // 64)
                def _(i):
                    here = pl.ds(pl.multiple_of(i * 64, 64), 64)
                    at = pl.ds(pl.multiple_of(r * rows + i * 64, 64), 64)
                    total = part[at, pl.ds(start, piece)].astype(F32) + pair_recv[r, 0, here, inside].astype(F32)
                    for far in range(1, chips):
                        total = total + far_recv[r, far, here, inside].astype(F32)
                    second = first_full[at, pl.ds(start, piece)].astype(F32) + total
                    squares = second * second
                    folded = squares[:, :128]
                    for lane_block in range(1, piece // 128):
                        folded = folded + squares[:, lane_block * 128 : (lane_block + 1) * 128]
                    sq_acc[at, :] += folded
                    if r == 0:
                        second_own[here, inside] = second
                    else:
                        returned[here, inside] = second.astype(BF16)

                if r == 1:
                    pl.when(has_guest)(lambda: back_copy(slot, guest).start())

    guest = lax.select(f == 1, 0, n - 1)

    def ahead_of(k):
        return lax.rem(t + k, n_tp)

    def square_copy(k, peer):
        return pltpu.make_async_remote_copy(
            src_ref=sq_send.at[0], dst_ref=sq_recv.at[0, k], send_sem=sq_ss.at[0, k],
            recv_sem=sq_rs.at[0, k], device_id={"tp": peer}, device_id_type=MESH,
        )

    def edge_squares(k, peer):
        return pltpu.make_async_remote_copy(
            src_ref=sq_send.at[1], dst_ref=sq_recv.at[1, k], send_sem=sq_ss.at[1, k],
            recv_sem=sq_rs.at[1, k], device_id={"fs": guest, "tp": peer}, device_id_type=MESH,
        )

    def squares_of(r):
        for i in range(seqs):
            at = pl.ds(r * rows + i * length, length)
            sums = jnp.sum(jnp.transpose(sq_acc[at, :]), axis=0, keepdims=True)
            sq_send[r, i : i + 1, :] = sums

    def squares_total():
        total = sq_send[0]
        for k in range(1, n_tp):
            square_copy(k, t).wait_recv()
            total = total + sq_recv[0, k]
        return total

    def put_out(i):
        at = pl.ds(i * length, length)
        return pltpu.make_async_copy(out_ref.at[at, :], out_hbm.at[at, :], out_sem.at[i])

    def close(values, squares):
        gain = out_gain[:, own_columns(t)]
        for i in range(seqs):
            factor = spread(lax.rsqrt(squares[i : i + 1, :] / width + 1e-06))
            inside = pl.ds(i * length, length)
            for start in range(0, columns, length):
                at = pl.ds(start, min(length, columns - start))
                scaled = values[inside, at].astype(F32) * factor[:, : at.size] * gain[:, start : start + at.size]
                out_ref[inside, at] = scaled.astype(BF16)
            put_out(i).start()

    has_guest = (f == 1) | (f == n - 2)
    inward = lax.select(f == 0, 1, n - 2)

    def tokens_in(device):
        return pltpu.make_async_remote_copy(
            src_ref=tok_ref, dst_ref=block_of(tok_full, 1, t), send_sem=guest_sem.at[0], recv_sem=guest_sem.at[1],
            device_id={"fs": device}, device_id_type=MESH,
        )

    @pl.when(jnp.logical_not(is_host))
    def _():
        small_copy(3).wait()
        order = [("own", w, c) for w in range(MIXER) for c in range(counts[w])] + [("tokens", 0, 0)]
        order += [("other", w, c) for w in range(MIXER) if direct(w) for c in range(counts[w])]
        for c in range(counts[GATE] + TRAIL):
            order += [("own", GATE, c)] if c < counts[GATE] else []
            order += [("other", GATE, c - TRAIL)] if c >= TRAIL else []
        for kind in ("own", "other"):
            order += [(kind, DOWN, c) for c in range(pieces)]
        for kind, w, c in order:
            if kind == "own":
                start_own(w, c)
            elif kind == "tokens":
                tokens_in(inward).start()
            else:
                start_other(w, c)
        tokens_in(inward).wait_send()
        for w in groups:
            z_sent(w, f, lax.select(f == 0, 1, -1))
            if direct(w):
                for k in range(1, parts):
                    y_sent(w, f, k)
        def take_back(slot):
            back_copy(slot, inward).wait_recv()

        def take_squares(k):
            edge_squares(k, t).wait_recv()

        for slot in range(columns // piece):
            take_back(slot)
        for k in range(n_tp):
            take_squares(k)
        sq_total[...] = sum(sq_recv[1, k] for k in range(1, n_tp)) + sq_recv[1, 0]
        close(returned, sq_total)

    @pl.when(is_host)
    def _():
        mixer_tiles = [(w, c) for w in range(MIXER) for c in range(counts[w])]
        for w, c in mixer_tiles:
            start_own(w, c)
        for w in range(7):
            own_copy(w).start()
        own_tokens().wait()
        gather_send(tok_full, 0, 0)
        for i in range(4):
            small_copy(i).wait()
        sq_acc[...] = jnp.zeros_like(sq_acc)
        sq_send[...] = jnp.zeros_like(sq_send)
        for w, c in mixer_tiles:
            from_inner(w, c)
            from_outer(w, c)
        last = counts[GATE] - 1

        def start_pair(c):
            if c <= last:
                start_own(GATE, c)

        def inner_pair(c):
            if c <= last:
                from_inner(GATE, c)

        def outer_pair(c):
            if c <= last:
                from_outer(GATE, c)

        def far_pair(c):
            if c <= last:
                from_far(GATE, c)

        def start_down(first, end):
            for c in range(first, min(end, pieces)):
                start_own(DOWN, c)

        def inner_down(c):
            if c < pieces:
                from_inner(DOWN, c)

        def outer_down(c):
            if c < pieces:
                from_outer(DOWN, c)

        def tile(c, r):
            if c <= last:
                if r == 0:
                    finish_all(GATE, c)
                hidden_tiles(c, r)

        def drain(group):
            for w in group:
                @pl.loop(0, n)
                def _(blk):
                    pl.when((f + 1 <= last_host) & (blk <= f))(lambda: z_sent(w, blk, 1))
                    pl.when((f - 1 >= first_host) & (blk >= f))(lambda: z_sent(w, blk, -1))
                    whole = ((blk == 0) & (f == 1)) | ((blk == n - 1) & (f == n - 2))
                    relayed = (blk != f) & jnp.logical_not(whole) if direct(w) else blk != f

                    @pl.when(relayed)
                    def _():
                        for k in range(1, parts):
                            y_sent(w, blk, k)

        start_pair(0)
        start_pair(1)
        start_pair(2)
        gather_relay(tok_full, 0, 0)
        for c in range(counts[0]):
            from_far(0, c)
        gather_finish(tok_full, 0, 0)
        norm_rows(tok_full, mix_gain, 0)
        for w, c in mixer_tiles[counts[0] :]:
            from_far(w, c)

        @pl.when(has_guest)
        def _():
            tokens_in(guest).wait_recv()

        gather_send(tok_full, 0, 1)
        inner_pair(0)
        for w in range(3):
            own_copy(w).wait()
            for c in range(counts[w]):
                finish_all(w, c)
            project(w, 0)
        convolve()
        own_copy(3).wait()
        finish_all(3, 0)
        mix(0)
        sum_send(0)
        inner_pair(1)
        gather_relay(tok_full, 0, 1)
        gather_finish(tok_full, 0, 1)
        outer_pair(0)
        sum_relay(0)
        norm_rows(tok_full, mix_gain, 1)
        inner_pair(2)
        project(0, 1)
        project(1, 1)
        outer_pair(1)
        start_pair(3)
        project(2, 1)
        convolve()
        mix(1)
        sum_send(1)
        far_pair(0)
        sum_relay(1)
        outer_pair(2)
        start_pair(4)
        far_pair(1)
        first_rows(0)
        gather_send(first_full, 2, 0)
        inner_pair(3)
        outer_pair(3)
        start_pair(5)
        far_pair(2)
        first_rows(1)
        gather_send(first_full, 2, 1)
        inner_pair(4)
        outer_pair(4)
        start_down(0, 1)
        far_pair(3)
        for w in (GATE, UP):
            own_copy(w).wait()
        gather_relay(first_full, 2, 0)
        inner_pair(5)
        gather_finish(first_full, 2, 0)
        outer_pair(5)
        start_down(1, pieces)
        norm_rows(first_full, ffn_gain, 0)
        far_pair(4)
        tile(0, 0)
        tile(1, 0)
        far_pair(5)
        tile(2, 0)
        gather_relay(first_full, 2, 1)
        tile(3, 0)
        inner_down(0)
        gather_finish(first_full, 2, 1)
        norm_rows(first_full, ffn_gain, 1)
        for r in range(2):
            for k in range(chips):
                to_pair(r, k).wait_send()
            for k in range(1, chips):
                to_far(r, k).wait_send()
        tile(0, 1)
        tile(1, 1)
        inner_down(1)
        tile(2, 1)
        tile(3, 1)
        inner_down(2)
        tile(4, 0)
        outer_down(0)
        tile(4, 1)
        tile(5, 0)
        inner_down(3)
        outer_down(1)
        tile(5, 1)
        for c in range(6, last + 1):
            start_pair(c)
            inner_pair(c)
            outer_pair(c)
            far_pair(c)
            tile(c, 0)
            tile(c, 1)
        own_copy(DOWN).wait()
        near, outer = f + inner, f - inner
        batch = 2 if pieces % 2 == 0 else 1

        def produce(b, first, count):
            for r in (1, 0):
                down_product(b, r, pl.multiple_of(first * piece, 128), count * piece)
            for i in range(count):
                to_lane(b, first + i)

        def far_down(c):
            if c < pieces:
                from_far(DOWN, c)

        def join(b, first, count):
            for c in range(first, first + count):
                combine(b, c)

        def take(b, first, count):
            for c in range(first, first + count):
                finish(DOWN, c, b)
            produce(b, first, count)

        def near_pieces(first, count):
            take(near, first, count)

        produce(f, 0, batch)
        near_pieces(0, batch)
        outer_down(2)
        join(f, 0, batch)
        join(near, 0, batch)
        far_down(0)
        for first in range(batch, pieces, batch):
            produce(f, first, batch)
            near_pieces(first, batch)
            join(f, first, batch)
            join(near, first, batch)
        far_down(1)
        for c in range(3, pieces):
            outer_down(c)
        take(outer, 0, 1)
        far_down(2)
        drain(groups[:-1])
        for r in range(2):
            gather_sent(tok_full, 0, r)
            gather_sent(first_full, 2, r)

        def others(visit):
            @pl.loop(1, n - 2)
            def _(s):
                for toward in (inner, -inner):
                    b = f + toward * (1 + s)
                    pl.when((b >= 0) & (b < n))(lambda: visit(b))

        def settle_range(first, end):
            @pl.loop(first, end)
            def _(i):
                settle(f, i)
                settle(near, i)

        def far_take(c):
            others(lambda b: take(b, c, 1))

        def far_join(c):
            others(lambda b: combine(b, c))

        far_take(0)
        join(outer, 0, 1)
        far_join(0)
        for c in range(1, batch):
            take(outer, c, 1)
        for c in range(3, pieces):
            from_far(DOWN, c)
        for c in range(1, batch):
            far_take(c)
            join(outer, c, 1)
        settle_range(0, batch)
        for c in range(1, batch):
            far_join(c)
        for c in range(batch, pieces):
            take(outer, c, 1)
            if c > batch:
                far_join(c - 1)
            join(outer, c, 1)
            if c == batch:
                settle_range(batch, pieces)
            if c + 1 == pieces:
                for i in range(batch):
                    settle(outer, i)
            far_take(c)
        if pieces > batch:
            far_join(pieces - 1)
        for c in range(pieces):
            others(lambda b: settle(b, c))
            if c >= batch or pieces == batch:
                settle(outer, c)

        squares_of(1)

        @pl.when(has_guest)
        def _():
            for k in range(n_tp):
                edge_squares(k, ahead_of(k)).start()

        squares_of(0)
        for k in range(1, n_tp):
            square_copy(k, ahead_of(k)).start()
        sq_total[...] = squares_total()
        close(second_own, sq_total)

        @pl.when(has_guest)
        def _():
            for k in range(n_tp):
                edge_squares(k, ahead_of(k)).wait_send()
            back_sent()

        for k in range(1, n_tp):
            square_copy(k, ahead_of(k)).wait_send()
        for r in range(2):
            for k in range(chips):
                down_sent(r, k)
        drain((DOWN,))

    for i in range(seqs):
        put_out(i).wait()


def solution(mesh):
    n, parts, n_tp = mesh.shape["fs"], mesh.shape["grp"], mesh.shape["tp"]

    def local(tokens, mix_gain, outer, inner, value, taps, mix_out, ffn_gain, gate, up, down, out_gain):
        seqs, length, columns = tokens.shape
        rows, width = seqs * length, columns * n_tp
        weights = (outer, inner, value, mix_out, gate, up, down)
        piece = min(down.shape[1], columns, 128)
        spans = [((0, a.shape[1]),) for a in weights]
        if outer.shape[1] % 256 == 0:
            spans[0] = ((0, outer.shape[1] // 2), (outer.shape[1] // 2, outer.shape[1] // 2))
        spans[GATE] = spans[UP] = tiles_of(gate.shape[1])
        spans[DOWN] = tuple((start, piece) for start in range(0, down.shape[1], piece))
        slots = sum(len(tiles) for w, tiles in enumerate(spans) if w != UP)
        groups = len(weights) - 1
        channels, units = outer.shape[1], gate.shape[1]
        y_others = max(parts - 1, 1)
        per_owner, packed = columns // piece, -(-seqs // 8) * 8
        dma = pltpu.SemaphoreType.DMA
        scratch = [pltpu.VMEM((n,) + a.shape, BF16) for a in weights[:GATE]]
        scratch += [pltpu.VMEM((2, n) + gate.shape, BF16), pltpu.VMEM((n,) + down.shape, BF16)]
        chips = n_tp // 2
        scratch += [
            pltpu.VMEM((2 * rows, width), BF16),
            pltpu.VMEM((2 * rows, width), BF16),
            pltpu.VMEM((3, rows, channels), BF16),
            pltpu.VMEM((rows, channels), BF16),
            pltpu.VMEM((2 * rows, width), BF16),
            pltpu.VMEM((2, chips, rows, columns), BF16),
            pltpu.VMEM((2, chips, rows, columns), BF16),
            pltpu.VMEM((2 * rows, width), BF16),
            pltpu.VMEM((2 * rows, units), BF16),
            pltpu.VMEM((rows, columns), BF16),
            pltpu.VMEM((rows, columns), F32),
            pltpu.VMEM((2 * rows, 128), F32),
            pltpu.VMEM((2, packed, length), F32),
            pltpu.VMEM((2, n_tp, packed, length), F32),
            pltpu.VMEM((packed, length), F32),
            pltpu.VMEM((rows, columns), BF16),
            pltpu.VMEM((1, width), F32), pltpu.VMEM(taps.shape, F32),
            pltpu.VMEM((1, width), F32), pltpu.VMEM((1, width), F32),
            dma((groups, n + 1)), dma((slots, n - 1)),
            dma((groups, n, y_others)), dma((slots, n - 1, y_others)),
            dma((12,)), dma((3, 2, chips)), dma((3, 2, chips)), dma((3, 2, chips)), dma((3, 2, chips)),
            dma((2, chips)), dma((2, chips, per_owner)), dma((2, chips)), dma((2, chips, per_owner)),
            dma((2, n_tp)), dma((2, n_tp)), dma((1,)), dma((per_owner,)), dma((2,)), dma((seqs,)),
        ]
        out = pl.pallas_call(
            functools.partial(kernel, n, parts, n_tp, length, tuple(spans)),
            out_shape=jax.ShapeDtypeStruct((rows, columns), BF16),
            in_specs=[pl.BlockSpec(memory_space=pl.ANY)] * 12,
            out_specs=pl.BlockSpec(memory_space=pl.ANY),
            scratch_shapes=scratch,
            compiler_params=pltpu.CompilerParams(
                collective_id=0, has_side_effects=True, vmem_limit_bytes=62 * 1024 * 1024
            ),
        )(
            tokens.reshape(rows, columns), mix_gain[None], outer, inner, value, taps, mix_out,
            ffn_gain[None], gate, up, down, out_gain[None],
        )
        return out.reshape(seqs, length, columns)

    in_specs = (
        P(("grp", "fs"), None, "tp"), P(), P("fs", "tp"), P("fs", "tp"), P("fs", "tp"), P(), P("tp", "fs"),
        P(), P("fs", "tp"), P("fs", "tp"), P("tp", "fs"), P(),
    )
    out_specs = P(("grp", "fs"), None, "tp")
    return jax.shard_map(local, mesh=mesh, in_specs=in_specs, out_specs=out_specs, check_vma=False)
```

```python
import functools

import jax
import jax.numpy as jnp
from jax import lax
from jax.experimental import pallas as pl
from jax.experimental.pallas import tpu as pltpu
from jax.sharding import PartitionSpec as P

MESH = pl.DeviceIdType.MESH
F32 = jnp.float32
BF16 = jnp.bfloat16
MIXER = 4
GATE, UP, DOWN = 4, 5, 6
SHARED = 2
TRAIL = 2
LAG = 2


def tiles_of(units):
    if units % 128:
        return ((0, units),)
    return tuple((start, min(256, units - start)) for start in range(0, units, 256))


def spread(rows):
    return jnp.transpose(jnp.broadcast_to(rows, (rows.shape[1], rows.shape[1])))


def kernel(
    n, parts, n_tp, length, spans,
    tok_ref, mix_gain_in, w0, w1, w2, taps_in, w3, ffn_gain_in, w4, w5, w6, out_gain_in,
    out_hbm,
    f0, f1, f2, f3, pair_full, f6,
    tok_full, normed, proj, gated, part, pair_recv, far_recv, first_full, hidden, returned, second_own, sq_acc,
    sq_send, sq_recv, sq_total, out_ref, mix_gain, taps_ref, ffn_gain, out_gain,
    z_send, z_recv, y_send, y_recv, own_sem, pair_ss, pair_rs, far_ss, far_rs,
    down_pair_ss, down_pair_rs, down_far_ss, down_far_rs, sq_ss, sq_rs, back_ss, back_rs, guest_sem, out_sem,
):
    own = (w0, w1, w2, w3, w4, w5, w6)
    full = (f0, f1, f2, f3, pair_full.at[0], pair_full.at[1], f6)
    f, g, t = lax.axis_index("fs"), lax.axis_index("grp"), lax.axis_index("tp")
    rows, columns = tok_ref.shape
    width = columns * n_tp
    seqs = rows // length
    counts = [len(tiles) for tiles in spans]
    groups = (0, 1, 2, 3, GATE, DOWN)
    ranks = {w: i for i, w in enumerate(groups)}
    bases = {w: sum(counts[v] for v in groups[:i]) for w, i in ranks.items()}

    def y_peer(k):
        return lax.rem(g + k, parts)

    def tp_peer(k):
        return lax.rem(t + k, n_tp)

    def span(w, half, c):
        size = own[w].shape[0] // parts
        if isinstance(c, int):
            at = pl.ds(*spans[w][c])
        else:
            width_c = spans[w][0][1]
            at = pl.ds(pl.multiple_of(c * width_c, 128), width_c)
        return pl.ds(pl.multiple_of(half * size, 8), size), at

    def members(w):
        return (GATE, UP) if w == GATE else (w,)

    def region(w, blk, half, c):
        at_rows, at_cols = span(w, half, c)
        if w == GATE:
            return pair_full.at[:, blk, at_rows, at_cols]
        return full[w].at[blk, at_rows, at_cols]

    def landing(v, blk, half, c):
        at_rows, at_cols = span(v, half, c)
        if v in (GATE, UP):
            return pair_full.at[v - GATE, blk, at_rows, at_cols]
        return full[v].at[blk, at_rows, at_cols]

    def piece_of(w, half, c):
        at_rows, at_cols = span(w, half, c)
        return own[w].at[at_rows, at_cols]

    def small_copy(i):
        pairs = ((mix_gain_in, mix_gain), (taps_in, taps_ref), (ffn_gain_in, ffn_gain), (out_gain_in, out_gain))
        return pltpu.make_async_copy(*pairs[i], own_sem.at[8 + i])

    def own_tokens():
        mine = tok_full.at[pl.ds(0, rows), pl.ds(pl.multiple_of(t * columns, 128), columns)]
        return pltpu.make_async_copy(tok_ref, mine, own_sem.at[7])

    hosting = (f >= 1) & (f <= n - 2)
    small_copy(3).start()

    @pl.when(hosting)
    def _():
        own_tokens().start()
        for i in range(3):
            small_copy(i).start()

    barrier = pltpu.get_barrier_semaphore()
    for k in range(1, n_tp):
        pl.semaphore_signal(barrier, inc=1, device_id={"tp": tp_peer(k)}, device_id_type=MESH)
    for k in range(1, parts):
        pl.semaphore_signal(barrier, inc=1, device_id={"grp": y_peer(k)}, device_id_type=MESH)

    @pl.when(f < n - 1)
    def _():
        pl.semaphore_signal(barrier, inc=1, device_id={"fs": f + 1}, device_id_type=MESH)

    @pl.when(f > 0)
    def _():
        pl.semaphore_signal(barrier, inc=1, device_id={"fs": f - 1}, device_id_type=MESH)

    neighbours = lax.min(f, 1) + lax.min(n - 1 - f, 1)
    pl.semaphore_wait(barrier, n_tp - 1 + parts - 1 + neighbours)

    def z_slot(blk, step):
        return lax.select((blk == f) & (step < 0), n, blk)

    def half_block(w, blk):
        size = own[w].shape[0] // parts
        at_rows = pl.ds(pl.multiple_of(g * size, 8), size)
        if w == GATE:
            return pair_full.at[:, blk, at_rows, :]
        return full[w].at[blk, at_rows, :]

    def z_sent(w, blk, step):
        half = half_block(w, blk)
        pltpu.make_async_remote_copy(
            src_ref=half, dst_ref=half, send_sem=z_send.at[ranks[w], z_slot(blk, step)], recv_sem=z_recv.at[bases[w], 0],
            device_id={"fs": f + step}, device_id_type=MESH,
        ).wait_send()

    def y_sent(w, blk, k):
        half = half_block(w, blk)
        pltpu.make_async_remote_copy(
            src_ref=half, dst_ref=half, send_sem=y_send.at[ranks[w], blk, k - 1], recv_sem=y_recv.at[bases[w], 0, k - 1],
            device_id={"grp": y_peer(k)}, device_id_type=MESH,
        ).wait_send()

    def seat(blk, host):
        return blk - lax.select(blk > host, 1, 0)

    def z_copy(w, c, blk, src, dst, step, host):
        return pltpu.make_async_remote_copy(
            src_ref=src, dst_ref=dst, send_sem=z_send.at[ranks[w], z_slot(blk, step)],
            recv_sem=z_recv.at[bases[w] + c, seat(blk, host)],
            device_id={"fs": f + step}, device_id_type=MESH,
        )

    def y_copy(w, c, blk, half, k, peer):
        return pltpu.make_async_remote_copy(
            src_ref=region(w, blk, half, c), dst_ref=region(w, blk, half, c),
            send_sem=y_send.at[ranks[w], blk, k - 1], recv_sem=y_recv.at[bases[w] + c, seat(blk, f), k - 1],
            device_id={"grp": peer}, device_id_type=MESH,
        )

    first_host, last_host = 1, n - 2
    is_host = (f >= first_host) & (f <= last_host)
    inner = lax.select(2 * f + 1 < n, 1, -1)

    def start_own(w, c):
        def towards(step):
            for v in members(w):
                z_copy(w, c, f, piece_of(v, g, c), landing(v, f, g, c), step, f + step).start()

        pl.when(f + 1 <= last_host)(lambda: towards(1))
        pl.when(f - 1 >= first_host)(lambda: towards(-1))

    def start_other(w, c):
        inward = lax.select(f == 0, 1, n - 2)
        for k in range(1, parts):
            half = lax.rem(g + parts - k, parts)
            for v in members(w):
                pltpu.make_async_remote_copy(
                    src_ref=piece_of(v, half, c), dst_ref=landing(v, f, half, c),
                    send_sem=y_send.at[ranks[w], f, k - 1],
                    recv_sem=y_recv.at[bases[w] + c, seat(f, inward), k - 1],
                    device_id={"fs": inward}, device_id_type=MESH,
                ).start()

    def direct(w):
        return w >= SHARED

    def relay(w, c, s, toward, next_to_edge):
        blk = f + toward * (1 + s)
        step = -toward

        @pl.when((blk >= 0) & (blk < n))
        def _():
            here = region(w, blk, g, c)
            z_copy(w, c, blk, here, here, step, f).wait_recv()

            def share():
                for k in range(1, parts):
                    y_copy(w, c, blk, g, k, y_peer(k)).start()

            def onward():
                z_copy(w, c, blk, here, here, step, f + step).start()

            pl.when((f + step <= last_host) & (f + step >= first_host))(onward)
            if next_to_edge and direct(w):
                pl.when((blk > 0) & (blk < n - 1))(share)
            else:
                share()

    def from_inner(w, c):
        relay(w, c, 0, inner, True)

    def from_outer(w, c):
        relay(w, c, 0, -inner, True)

    def from_far(w, c):
        @pl.loop(1, n - 2)
        def _(s):
            relay(w, c, s, inner, False)
            relay(w, c, s, -inner, False)

    def finish(w, c, blk):
        for k in range(1, parts):
            source = lax.rem(g + parts - k, parts)
            y_copy(w, c, blk, source, k, source).wait_recv()

    def finish_all(w, c):
        @pl.loop(0, n)
        def _(blk):
            pl.when(blk != f)(lambda: finish(w, c, blk))

    def own_copy(w):
        return pltpu.make_async_copy(own[w], full[w].at[f], own_sem.at[w])

    def own_columns(owner):
        return pl.ds(pl.multiple_of(owner * columns, 128), columns)

    chips = n_tp // 2
    core = lax.rem(t, 2)
    pair = t + 1 - 2 * core

    def ahead(k, start=None):
        return lax.rem((t if start is None else start) + 2 * k, n_tp)

    def behind(k, start=None):
        return lax.rem((t if start is None else start) + n_tp - 2 * k, n_tp)

    def set_rows(r):
        return pl.ds(r * rows, rows)

    def pair_copy(stage, r, k, src, dst):
        return pltpu.make_async_remote_copy(
            src_ref=src, dst_ref=dst, send_sem=pair_ss.at[stage, r, k], recv_sem=pair_rs.at[stage, r, k],
            device_id={"tp": pair}, device_id_type=MESH,
        )

    def far_copy(stage, r, k, src, dst, peer):
        return pltpu.make_async_remote_copy(
            src_ref=src, dst_ref=dst, send_sem=far_ss.at[stage, r, k], recv_sem=far_rs.at[stage, r, k],
            device_id={"tp": peer}, device_id_type=MESH,
        )

    def block_of(buf, r, owner):
        return buf.at[set_rows(r), own_columns(owner)]

    def gather_send(buf, stage, r):
        mine = block_of(buf, r, t)
        for k in range(1, chips):
            far_copy(stage, r, k, mine, mine, ahead(k)).start()
        pair_copy(stage, r, 0, mine, mine).start()

    def gather_relay(buf, stage, r):
        for k in range(1, chips):
            theirs = block_of(buf, r, behind(k))
            far_copy(stage, r, k, theirs, theirs, behind(k)).wait_recv()
            pair_copy(stage, r, k, theirs, theirs).start()

    def gather_finish(buf, stage, r):
        for k in range(chips):
            theirs = block_of(buf, r, behind(k, pair))
            pair_copy(stage, r, k, theirs, theirs).wait_recv()

    def gather_sent(buf, stage, r):
        mine = block_of(buf, r, t)
        for k in range(1, chips):
            far_copy(stage, r, k, mine, mine, ahead(k)).wait_send()
        for k in range(chips):
            pair_copy(stage, r, k, mine, mine).wait_send()

    def to_pair(r, k):
        return pair_copy(1, r, k, block_of(part, r, ahead(k, pair)), pair_recv.at[r, k])

    def to_far(r, k):
        return far_copy(1, r, k, block_of(part, r, ahead(k)), far_recv.at[r, k], ahead(k))

    def sum_send(r):
        for k in range(chips - 1, -1, -1):
            to_pair(r, k).start()

    def sum_relay(r):
        for k in range(1, chips):
            to_pair(r, k).wait_recv()

            @pl.loop(0, rows // 64)
            def _(i):
                inside = pl.ds(pl.multiple_of(i * 64, 64), 64)
                at = pl.ds(pl.multiple_of(r * rows + i * 64, 64), 64)
                both = part[at, own_columns(ahead(k))].astype(F32) + pair_recv[r, k, inside, :].astype(F32)
                part[at, own_columns(ahead(k))] = both.astype(BF16)

            to_far(r, k).start()

    def summed(r, start, size):
        inside = pl.ds(pl.multiple_of(start, size), size)
        at = pl.ds(pl.multiple_of(r * rows + start, size), size)
        total = part[at, own_columns(t)].astype(F32) + pair_recv[r, 0, inside, :].astype(F32)
        for k in range(1, chips):
            total = total + far_recv[r, k, inside, :].astype(F32)
        return at, total

    def first_rows(r):
        to_pair(r, 0).wait_recv()
        for k in range(1, chips):
            to_far(r, k).wait_recv()

        @pl.loop(0, rows // 64)
        def _(i):
            at, total = summed(r, i * 64, 64)
            first_full[at, own_columns(t)] = (tok_full[at, own_columns(t)].astype(F32) + total).astype(BF16)

    def norm_rows(source, gain, r):
        size = 32

        @pl.loop(0, rows // size)
        def _(i):
            at = pl.ds(pl.multiple_of(r * rows + i * size, size), size)
            values = source[at, :].astype(F32)
            scale = lax.rsqrt(jnp.sum(values * values, axis=1, keepdims=True) / width + 1e-06)
            normed[at, :] = (values * scale * gain[...]).astype(BF16)

    channels = w0.shape[1]
    block = w3.shape[1]
    units = w4.shape[1]
    tap_count = taps_ref.shape[0]

    def project(w, r):
        weight = full[w][...].reshape(width, channels)
        proj[w] = jnp.dot(normed[set_rows(r), :], weight, preferred_element_type=F32).astype(BF16)

    def convolve():
        taps = taps_ref[:, pl.ds(pl.multiple_of(t * channels, 128), channels)]

        @pl.loop(0, seqs)
        def _(i):
            at = pl.ds(pl.multiple_of(i * length, length), length)
            product = proj[1, at, :].astype(F32) * proj[2, at, :].astype(F32)
            position = lax.broadcasted_iota(jnp.int32, product.shape, 0)
            conv = jnp.zeros_like(product)
            for offset in range(tap_count):
                shift = tap_count - 1 - offset
                moved = product if shift == 0 else jnp.where(position >= shift, pltpu.roll(product, shift, 0), 0.0)
                conv = conv + taps[offset : offset + 1, :] * moved
            gated[at, :] = (proj[0, at, :].astype(F32) * conv).astype(BF16)

    def mix(r):
        @pl.loop(0, n)
        def _(b):
            at = pl.ds(pl.multiple_of(b * block, 128), block)
            part[set_rows(r), at] = jnp.dot(gated[...], full[3][b], preferred_element_type=F32).astype(BF16)

    def hidden_tile(r, start, size):
        at = pl.ds(start, size)
        left = normed[set_rows(r), :]
        gate = jnp.dot(left, full[GATE][:, :, at].reshape(width, size), preferred_element_type=F32)
        upward = jnp.dot(left, full[UP][:, :, at].reshape(width, size), preferred_element_type=F32)
        hidden[set_rows(r), at] = (gate / (1.0 + jnp.exp(-gate)) * upward).astype(BF16)

    def hidden_tiles(c, r):
        first, total = spans[GATE][c]
        for offset in range(0, total, 256):
            hidden_tile(r, first + offset, min(256, total - offset))

    wide = w6.shape[1]
    piece = spans[DOWN][0][1]
    pieces = counts[DOWN]

    def down_to_pair(r, k, slot, start):
        inside = pl.ds(pl.multiple_of(slot * piece, 128), piece)
        return pltpu.make_async_remote_copy(
            src_ref=part.at[set_rows(r), pl.ds(start, piece)], dst_ref=pair_recv.at[r, k, :, inside],
            send_sem=down_pair_ss.at[r, k], recv_sem=down_pair_rs.at[r, k, slot],
            device_id={"tp": pair}, device_id_type=MESH,
        )

    def down_to_far(r, k, slot, start):
        inside = pl.ds(pl.multiple_of(slot * piece, 128), piece)
        return pltpu.make_async_remote_copy(
            src_ref=part.at[set_rows(r), pl.ds(start, piece)], dst_ref=far_recv.at[r, k, :, inside],
            send_sem=down_far_ss.at[r, k], recv_sem=down_far_rs.at[r, k, slot],
            device_id={"tp": lax.rem(t + 2 * k, n_tp)}, device_id_type=MESH,
        )

    def down_sent(r, k):
        whole = pair_recv.at[r, k]
        pltpu.make_async_remote_copy(
            src_ref=whole, dst_ref=whole, send_sem=down_pair_ss.at[r, k], recv_sem=down_pair_rs.at[r, k, 0],
            device_id={"tp": pair}, device_id_type=MESH,
        ).wait_send()
        if k > 0:
            pltpu.make_async_remote_copy(
                src_ref=whole, dst_ref=whole, send_sem=down_far_ss.at[r, k], recv_sem=down_far_rs.at[r, k, 0],
                device_id={"tp": lax.rem(t + 2 * k, n_tp)}, device_id_type=MESH,
            ).wait_send()

    def place(b, c):
        start = pl.multiple_of(b * wide + c * piece, 128)
        owner = (b * wide + c * piece) // columns
        slot = lax.rem(b * wide + c * piece, columns) // piece
        k = lax.rem(owner // 2 - t // 2 + chips, chips)
        return start, owner, slot, k, lax.rem(owner, 2) == core

    def down_product(b, r, offset, size):
        weight = full[DOWN][b, :, pl.ds(offset, size)]
        part[set_rows(r), pl.ds(pl.multiple_of(b * wide + offset, 128), size)] = jnp.dot(
            hidden[set_rows(r), :], weight, preferred_element_type=F32
        ).astype(BF16)

    def to_lane(b, c):
        start, owner, slot, k, lane = place(b, c)

        @pl.when(jnp.logical_not(lane))
        def _():
            for r in (1, 0):
                down_to_pair(r, k, slot, start).start()

    def combine(b, c):
        start, owner, slot, k, lane = place(b, c)

        @pl.when(lane & (k > 0))
        def _():
            inside = pl.ds(pl.multiple_of(slot * piece, 128), piece)
            for r in (1, 0):
                down_to_pair(r, k, slot, start).wait_recv()

                @pl.loop(0, rows // 64)
                def _(i):
                    here = pl.ds(pl.multiple_of(i * 64, 64), 64)
                    at = pl.ds(pl.multiple_of(r * rows + i * 64, 64), 64)
                    both = part[at, pl.ds(start, piece)].astype(F32) + pair_recv[r, k, here, inside].astype(F32)
                    part[at, pl.ds(start, piece)] = both.astype(BF16)

                down_to_far(r, k, slot, start).start()

    def back_copy(slot, device):
        at = pl.ds(pl.multiple_of(slot * piece, 128), piece)
        return pltpu.make_async_remote_copy(
            src_ref=returned.at[:, at], dst_ref=returned.at[:, at], send_sem=back_ss.at[0], recv_sem=back_rs.at[slot],
            device_id={"fs": device}, device_id_type=MESH,
        )

    def back_sent():
        pltpu.make_async_remote_copy(
            src_ref=returned, dst_ref=returned, send_sem=back_ss.at[0], recv_sem=back_rs.at[0],
            device_id={"fs": guest}, device_id_type=MESH,
        ).wait_send()

    def settle(b, c):
        start, owner, slot, k, lane = place(b, c)

        @pl.when(owner == t)
        def _():
            inside = pl.ds(pl.multiple_of(slot * piece, 128), piece)
            for r in (1, 0):
                down_to_pair(r, 0, slot, start).wait_recv()
                for far in range(1, chips):
                    down_to_far(r, far, slot, start).wait_recv()

                @pl.loop(0, rows // 64)
                def _(i):
                    here = pl.ds(pl.multiple_of(i * 64, 64), 64)
                    at = pl.ds(pl.multiple_of(r * rows + i * 64, 64), 64)
                    total = part[at, pl.ds(start, piece)].astype(F32) + pair_recv[r, 0, here, inside].astype(F32)
                    for far in range(1, chips):
                        total = total + far_recv[r, far, here, inside].astype(F32)
                    second = first_full[at, pl.ds(start, piece)].astype(F32) + total
                    squares = second * second
                    folded = squares[:, :128]
                    for lane_block in range(1, piece // 128):
                        folded = folded + squares[:, lane_block * 128 : (lane_block + 1) * 128]
                    sq_acc[at, :] += folded
                    if r == 0:
                        second_own[here, inside] = second
                    else:
                        returned[here, inside] = second.astype(BF16)

                if r == 1:
                    pl.when(has_guest)(lambda: back_copy(slot, guest).start())

    guest = lax.select(f == 1, 0, n - 1)

    def ahead_of(k):
        return lax.rem(t + k, n_tp)

    def square_copy(k, peer):
        return pltpu.make_async_remote_copy(
            src_ref=sq_send.at[0], dst_ref=sq_recv.at[0, k], send_sem=sq_ss.at[0, k],
            recv_sem=sq_rs.at[0, k], device_id={"tp": peer}, device_id_type=MESH,
        )

    def edge_squares(k, peer):
        return pltpu.make_async_remote_copy(
            src_ref=sq_send.at[1], dst_ref=sq_recv.at[1, k], send_sem=sq_ss.at[1, k],
            recv_sem=sq_rs.at[1, k], device_id={"fs": guest, "tp": peer}, device_id_type=MESH,
        )

    def squares_of(r):
        for i in range(seqs):
            at = pl.ds(r * rows + i * length, length)
            sums = jnp.sum(jnp.transpose(sq_acc[at, :]), axis=0, keepdims=True)
            sq_send[r, i : i + 1, :] = sums

    def squares_total():
        total = sq_send[0]
        for k in range(1, n_tp):
            square_copy(k, t).wait_recv()
            total = total + sq_recv[0, k]
        return total

    def put_out(i):
        at = pl.ds(i * length, length)
        return pltpu.make_async_copy(out_ref.at[at, :], out_hbm.at[at, :], out_sem.at[i])

    def close(values, squares):
        gain = out_gain[:, own_columns(t)]
        for i in range(seqs):
            factor = spread(lax.rsqrt(squares[i : i + 1, :] / width + 1e-06))
            inside = pl.ds(i * length, length)
            for start in range(0, columns, length):
                at = pl.ds(start, min(length, columns - start))
                scaled = values[inside, at].astype(F32) * factor[:, : at.size] * gain[:, start : start + at.size]
                out_ref[inside, at] = scaled.astype(BF16)
            put_out(i).start()

    has_guest = (f == 1) | (f == n - 2)
    inward = lax.select(f == 0, 1, n - 2)

    def tokens_in(device):
        return pltpu.make_async_remote_copy(
            src_ref=tok_ref, dst_ref=block_of(tok_full, 1, t), send_sem=guest_sem.at[0], recv_sem=guest_sem.at[1],
            device_id={"fs": device}, device_id_type=MESH,
        )

    @pl.when(jnp.logical_not(is_host))
    def _():
        small_copy(3).wait()
        order = [("own", w, c) for w in range(MIXER) for c in range(counts[w])] + [("tokens", 0, 0)]
        order += [("other", w, c) for w in range(MIXER) if direct(w) for c in range(counts[w])]
        for c in range(counts[GATE] + TRAIL):
            order += [("own", GATE, c)] if c < counts[GATE] else []
            order += [("other", GATE, c - TRAIL)] if c >= TRAIL else []
        for kind in ("own", "other"):
            order += [(kind, DOWN, c) for c in range(pieces)]
        for kind, w, c in order:
            if kind == "own":
                start_own(w, c)
            elif kind == "tokens":
                tokens_in(inward).start()
            else:
                start_other(w, c)
        tokens_in(inward).wait_send()
        for w in groups:
            z_sent(w, f, lax.select(f == 0, 1, -1))
            if direct(w):
                for k in range(1, parts):
                    y_sent(w, f, k)
        def take_back(slot):
            back_copy(slot, inward).wait_recv()

        def take_squares(k):
            edge_squares(k, t).wait_recv()

        for slot in range(columns // piece):
            take_back(slot)
        for k in range(n_tp):
            take_squares(k)
        sq_total[...] = sum(sq_recv[1, k] for k in range(1, n_tp)) + sq_recv[1, 0]
        close(returned, sq_total)

    @pl.when(is_host)
    def _():
        mixer_tiles = [(w, c) for w in range(MIXER) for c in range(counts[w])]
        for w, c in mixer_tiles:
            start_own(w, c)
        for w in range(7):
            own_copy(w).start()
        own_tokens().wait()
        gather_send(tok_full, 0, 0)
        for i in range(4):
            small_copy(i).wait()
        sq_acc[...] = jnp.zeros_like(sq_acc)
        sq_send[...] = jnp.zeros_like(sq_send)
        for w, c in mixer_tiles:
            from_inner(w, c)
            from_outer(w, c)
        last = counts[GATE] - 1

        def start_pair(c):
            if c <= last:
                start_own(GATE, c)

        def inner_pair(c):
            if c <= last:
                from_inner(GATE, c)

        def outer_pair(c):
            if c <= last:
                from_outer(GATE, c)

        def far_pair(c):
            if c <= last:
                from_far(GATE, c)

        def start_down(first, end):
            for c in range(first, min(end, pieces)):
                start_own(DOWN, c)

        def inner_down(c):
            if c < pieces:
                from_inner(DOWN, c)

        def outer_down(c):
            if c < pieces:
                from_outer(DOWN, c)

        def tile(c, r):
            if c <= last:
                if r == 0:
                    finish_all(GATE, c)
                hidden_tiles(c, r)

        def drain(group):
            for w in group:
                @pl.loop(0, n)
                def _(blk):
                    pl.when((f + 1 <= last_host) & (blk <= f))(lambda: z_sent(w, blk, 1))
                    pl.when((f - 1 >= first_host) & (blk >= f))(lambda: z_sent(w, blk, -1))
                    whole = ((blk == 0) & (f == 1)) | ((blk == n - 1) & (f == n - 2))
                    relayed = (blk != f) & jnp.logical_not(whole) if direct(w) else blk != f

                    @pl.when(relayed)
                    def _():
                        for k in range(1, parts):
                            y_sent(w, blk, k)

        start_pair(0)
        start_pair(1)
        start_pair(2)
        gather_relay(tok_full, 0, 0)
        for c in range(counts[0]):
            from_far(0, c)
        gather_finish(tok_full, 0, 0)
        norm_rows(tok_full, mix_gain, 0)
        for w, c in mixer_tiles[counts[0] :]:
            from_far(w, c)

        @pl.when(has_guest)
        def _():
            tokens_in(guest).wait_recv()

        gather_send(tok_full, 0, 1)
        inner_pair(0)
        for w in range(3):
            own_copy(w).wait()
            for c in range(counts[w]):
                finish_all(w, c)
            project(w, 0)
        convolve()
        own_copy(3).wait()
        finish_all(3, 0)
        mix(0)
        sum_send(0)
        inner_pair(1)
        gather_relay(tok_full, 0, 1)
        gather_finish(tok_full, 0, 1)
        outer_pair(0)
        sum_relay(0)
        norm_rows(tok_full, mix_gain, 1)
        inner_pair(2)
        project(0, 1)
        project(1, 1)
        outer_pair(1)
        start_pair(3)
        project(2, 1)
        convolve()
        mix(1)
        sum_send(1)
        far_pair(0)
        sum_relay(1)
        outer_pair(2)
        start_pair(4)
        far_pair(1)
        first_rows(0)
        gather_send(first_full, 2, 0)
        inner_pair(3)
        outer_pair(3)
        start_pair(5)
        far_pair(2)
        first_rows(1)
        gather_send(first_full, 2, 1)
        inner_pair(4)
        outer_pair(4)
        start_down(0, 1)
        far_pair(3)
        for w in (GATE, UP):
            own_copy(w).wait()
        gather_relay(first_full, 2, 0)
        inner_pair(5)
        gather_finish(first_full, 2, 0)
        outer_pair(5)
        start_down(1, pieces)
        norm_rows(first_full, ffn_gain, 0)
        far_pair(4)
        tile(0, 0)
        tile(1, 0)
        far_pair(5)
        tile(2, 0)
        gather_relay(first_full, 2, 1)
        tile(3, 0)
        inner_down(0)
        gather_finish(first_full, 2, 1)
        norm_rows(first_full, ffn_gain, 1)
        for r in range(2):
            for k in range(chips):
                to_pair(r, k).wait_send()
            for k in range(1, chips):
                to_far(r, k).wait_send()
        tile(0, 1)
        tile(1, 1)
        inner_down(1)
        tile(2, 1)
        tile(3, 1)
        inner_down(2)
        tile(4, 0)
        outer_down(0)
        tile(4, 1)
        tile(5, 0)
        inner_down(3)
        outer_down(1)
        tile(5, 1)
        for c in range(6, last + 1):
            start_pair(c)
            inner_pair(c)
            outer_pair(c)
            far_pair(c)
            tile(c, 0)
            tile(c, 1)
        own_copy(DOWN).wait()
        near, outer = f + inner, f - inner
        batch = 2 if pieces % 2 == 0 else 1

        def produce(b, first, count):
            for r in (1, 0):
                down_product(b, r, pl.multiple_of(first * piece, 128), count * piece)
            for i in range(count):
                to_lane(b, first + i)

        def far_down(c):
            if c < pieces:
                from_far(DOWN, c)

        def join(b, first, count):
            for c in range(first, first + count):
                combine(b, c)

        def take(b, first, count):
            for c in range(first, first + count):
                finish(DOWN, c, b)
            produce(b, first, count)

        def near_pieces(first, count):
            take(near, first, count)

        produce(f, 0, batch)
        near_pieces(0, batch)
        outer_down(2)
        join(f, 0, batch)
        join(near, 0, batch)
        far_down(0)
        for first in range(batch, pieces, batch):
            produce(f, first, batch)
            near_pieces(first, batch)
            join(f, first, batch)
            join(near, first, batch)
        far_down(1)
        for c in range(3, pieces):
            outer_down(c)
        take(outer, 0, 1)
        far_down(2)
        drain(groups[:-1])
        for r in range(2):
            gather_sent(tok_full, 0, r)
            gather_sent(first_full, 2, r)

        def others(visit):
            @pl.loop(1, n - 2)
            def _(s):
                for toward in (inner, -inner):
                    b = f + toward * (1 + s)
                    pl.when((b >= 0) & (b < n))(lambda: visit(b))

        def settle_range(first, end):
            @pl.loop(first, end)
            def _(i):
                settle(f, i)
                settle(near, i)

        def far_take(c):
            others(lambda b: take(b, c, 1))

        def far_join(c):
            others(lambda b: combine(b, c))

        far_take(0)
        join(outer, 0, 1)
        far_join(0)
        for c in range(1, batch):
            take(outer, c, 1)
        for c in range(3, pieces):
            from_far(DOWN, c)
        for c in range(1, batch):
            far_take(c)
            join(outer, c, 1)
        settle_range(0, batch)
        for c in range(1, batch):
            far_join(c)
        for c in range(batch, pieces):
            take(outer, c, 1)
            if c > batch:
                far_join(c - 1)
            join(outer, c, 1)
            if c == batch:
                settle_range(batch, pieces)
            if c + 1 == pieces:
                for i in range(batch):
                    settle(outer, i)
            far_take(c)
        if pieces > batch:
            far_join(pieces - 1)
        for c in range(pieces):
            others(lambda b: settle(b, c))
            if c >= batch or pieces == batch:
                settle(outer, c)

        squares_of(1)

        @pl.when(has_guest)
        def _():
            for k in range(n_tp):
                edge_squares(k, ahead_of(k)).start()

        squares_of(0)
        for k in range(1, n_tp):
            square_copy(k, ahead_of(k)).start()
        sq_total[...] = squares_total()
        close(second_own, sq_total)

        @pl.when(has_guest)
        def _():
            for k in range(n_tp):
                edge_squares(k, ahead_of(k)).wait_send()
            back_sent()

        for k in range(1, n_tp):
            square_copy(k, ahead_of(k)).wait_send()
        for r in range(2):
            for k in range(chips):
                down_sent(r, k)
        drain((DOWN,))

    for i in range(seqs):
        put_out(i).wait()


def solution(mesh):
    n, parts, n_tp = mesh.shape["fs"], mesh.shape["grp"], mesh.shape["tp"]

    def local(tokens, mix_gain, outer, inner, value, taps, mix_out, ffn_gain, gate, up, down, out_gain):
        seqs, length, columns = tokens.shape
        rows, width = seqs * length, columns * n_tp
        weights = (outer, inner, value, mix_out, gate, up, down)
        piece = min(down.shape[1], columns, 128)
        spans = [((0, a.shape[1]),) for a in weights]
        if outer.shape[1] % 256 == 0:
            spans[0] = ((0, outer.shape[1] // 2), (outer.shape[1] // 2, outer.shape[1] // 2))
        spans[GATE] = spans[UP] = tiles_of(gate.shape[1])
        spans[DOWN] = tuple((start, piece) for start in range(0, down.shape[1], piece))
        slots = sum(len(tiles) for w, tiles in enumerate(spans) if w != UP)
        groups = len(weights) - 1
        channels, units = outer.shape[1], gate.shape[1]
        y_others = max(parts - 1, 1)
        per_owner, packed = columns // piece, -(-seqs // 8) * 8
        dma = pltpu.SemaphoreType.DMA
        scratch = [pltpu.VMEM((n,) + a.shape, BF16) for a in weights[:GATE]]
        scratch += [pltpu.VMEM((2, n) + gate.shape, BF16), pltpu.VMEM((n,) + down.shape, BF16)]
        chips = n_tp // 2
        scratch += [
            pltpu.VMEM((2 * rows, width), BF16),
            pltpu.VMEM((2 * rows, width), BF16),
            pltpu.VMEM((3, rows, channels), BF16),
            pltpu.VMEM((rows, channels), BF16),
            pltpu.VMEM((2 * rows, width), BF16),
            pltpu.VMEM((2, chips, rows, columns), BF16),
            pltpu.VMEM((2, chips, rows, columns), BF16),
            pltpu.VMEM((2 * rows, width), BF16),
            pltpu.VMEM((2 * rows, units), BF16),
            pltpu.VMEM((rows, columns), BF16),
            pltpu.VMEM((rows, columns), F32),
            pltpu.VMEM((2 * rows, 128), F32),
            pltpu.VMEM((2, packed, length), F32),
            pltpu.VMEM((2, n_tp, packed, length), F32),
            pltpu.VMEM((packed, length), F32),
            pltpu.VMEM((rows, columns), BF16),
            pltpu.VMEM((1, width), F32), pltpu.VMEM(taps.shape, F32),
            pltpu.VMEM((1, width), F32), pltpu.VMEM((1, width), F32),
            dma((groups, n + 1)), dma((slots, n - 1)),
            dma((groups, n, y_others)), dma((slots, n - 1, y_others)),
            dma((12,)), dma((3, 2, chips)), dma((3, 2, chips)), dma((3, 2, chips)), dma((3, 2, chips)),
            dma((2, chips)), dma((2, chips, per_owner)), dma((2, chips)), dma((2, chips, per_owner)),
            dma((2, n_tp)), dma((2, n_tp)), dma((1,)), dma((per_owner,)), dma((2,)), dma((seqs,)),
        ]
        out = pl.pallas_call(
            functools.partial(kernel, n, parts, n_tp, length, tuple(spans)),
            out_shape=jax.ShapeDtypeStruct((rows, columns), BF16),
            in_specs=[pl.BlockSpec(memory_space=pl.ANY)] * 12,
            out_specs=pl.BlockSpec(memory_space=pl.ANY),
            scratch_shapes=scratch,
            compiler_params=pltpu.CompilerParams(
                collective_id=0, has_side_effects=True, vmem_limit_bytes=62 * 1024 * 1024
            ),
        )(
            tokens.reshape(rows, columns), mix_gain[None], outer, inner, value, taps, mix_out,
            ffn_gain[None], gate, up, down, out_gain[None],
        )
        return out.reshape(seqs, length, columns)

    in_specs = (
        P(("grp", "fs"), None, "tp"), P(), P("fs", "tp"), P("fs", "tp"), P("fs", "tp"), P(), P("tp", "fs"),
        P(), P("fs", "tp"), P("fs", "tp"), P("tp", "fs"), P(),
    )
    out_specs = P(("grp", "fs"), None, "tp")
    return jax.shard_map(local, mesh=mesh, in_specs=in_specs, out_specs=out_specs, check_vma=False)
```
